32 devices in a mesh: tp: 4 (over z), dp: 8 (over y, x, core).
Axes of the slice: x: 2, y: 2, z: 4, core: 2. Of those that a mesh axis runs over, the one named last changes fastest.
Arguments:
- tokens: bfloat16 [64, 4096], P(None, 'dp'), may hold values from -6 to 6
- norm_gain: float32 [2, 4096], P(None, 'dp'), may hold values from 0.1 to 1.9
- w_gate: bfloat16 [2, 4096, 3072], P(None, 'dp', 'tp'), may hold values from -0.09375 to 0.09375
- w_value: bfloat16 [2, 4096, 3072], P(None, 'dp', 'tp'), may hold values from -0.09375 to 0.09375
- w_inmap: bfloat16 [2, 4096, 3072], P(None, 'dp', 'tp'), may hold values from -0.09375 to 0.09375
- w_readout: bfloat16 [2, 4096, 3072], P(None, 'dp', 'tp'), may hold values from -0.09375 to 0.09375
- w_step: bfloat16 [2, 4096, 48], P(None, 'dp'), may hold values from -0.09375 to 0.09375
- step_bias: float32 [2, 48], P(None, 'tp'), may hold values from -4 to 1
- decay_log: float32 [2, 48], P(None, 'tp'), may hold values from -1 to 2.5
- skip_gain: float32 [2, 48], P(None, 'tp'), may hold values from 0.5 to 2
- conv_taps: bfloat16 [2, 5, 3, 3072], P(None, None, None, 'tp'), may hold values from -2.5 to 2.5
- gate_gain: float32 [2, 3072], P(None, 'tp'), may hold values from 0.1 to 1.9
- w_project: bfloat16 [2, 3072, 4096], P(None, 'tp', 'dp'), may hold values from -0.109375 to 0.109375
- states: float32 [2, 64, 48, 4096], P(None, 'dp', 'tp'), may hold values from -3 to 3
- recent: bfloat16 [2, 64, 4, 3, 3072], P(None, 'dp', None, None, 'tp'), may hold values from -6 to 6
Outputs:
- next_tokens: bfloat16 [64, 4096], P(None, 'dp')
- next_states: float32 [2, 64, 48, 4096], P(None, 'dp', 'tp')
- next_recent: bfloat16 [2, 64, 4, 3, 3072], P(None, 'dp', None, None, 'tp')
The draws below stay inside these ranges and needn't reach their ends.
All inputs are finite; a program needn't handle non-finite values.
Results may differ from the reference program's by a relative error of at most 0.014.
Values may be sent and summed in bfloat16 or wider, within the bound.
A program may use at most 64 MiB of HBM per device.

```python
import jax
import jax.numpy as jnp
from jax import lax

D = 4096
HEADS = 48
HEAD_DIM = 64
STATE = 64
SSD_DIM = 3072
CONV = 5
LAYERS = 2
BATCH = 64


def shard_levels(stream_key, extent, split, low, high):
    loudness = 1.0
    for position, shards_of in split:
        heights = jax.random.uniform(jax.random.fold_in(jax.random.fold_in(stream_key, 6), position), (shards_of,), jnp.float32, low / len(split), high / len(split))
        loudness = loudness * jnp.repeat(jnp.exp(heights), extent[position] // shards_of).reshape((-1,) + (1,) * (len(extent) - 1 - position))
    return loudness


def scatter_about(own_key, extent, deviation, bound, split=(), dtype=jnp.bfloat16):
    values = jax.random.normal(own_key, extent, jnp.float32) * deviation
    if len(split) > 0:
        values = shard_levels(own_key, extent, split, -0.22, 0.18) * values
    return jnp.clip(values, min=-bound, max=bound).astype(dtype)


def setup_inputs(seed: int = 0) -> dict:
    key_of = jax.random.split(jax.random.key(seed), 16)
    return {
        "tokens": scatter_about(key_of[0], (BATCH, D), 1.0, 6.0, ((1, 8),)),
        "norm_gain": jnp.clip(1.0 + 0.18 * jax.random.normal(key_of[1], (LAYERS, D), jnp.float32), 0.1, 1.9),
        "w_gate": scatter_about(key_of[2], (LAYERS, D, SSD_DIM), D ** -0.5, 0.09375, ((1, 8), (2, 4))),
        "w_value": scatter_about(key_of[3], (LAYERS, D, SSD_DIM), D ** -0.5, 0.09375, ((1, 8), (2, 4))),
        "w_inmap": scatter_about(key_of[4], (LAYERS, D, SSD_DIM), D ** -0.5, 0.09375, ((1, 8), (2, 4))),
        "w_readout": scatter_about(key_of[5], (LAYERS, D, SSD_DIM), D ** -0.5, 0.09375, ((1, 8), (2, 4))),
        "w_step": scatter_about(key_of[6], (LAYERS, D, HEADS), D ** -0.5, 0.09375, ((1, 8),)),
        "step_bias": jnp.clip(-4.0 + 5.0 * jax.random.uniform(key_of[7], (LAYERS, HEADS), jnp.float32) ** shard_levels(key_of[7], (LAYERS, HEADS), ((1, 4),), -0.2, 0.2), -4.0, 1.0),
        "decay_log": jnp.clip(-1.0 + 3.5 * jax.random.uniform(key_of[8], (LAYERS, HEADS), jnp.float32) ** shard_levels(key_of[8], (LAYERS, HEADS), ((1, 4),), -0.2, 0.2), -1.0, 2.5),
        "skip_gain": jnp.clip(0.5 + 1.5 * jax.random.uniform(key_of[9], (LAYERS, HEADS), jnp.float32) ** shard_levels(key_of[9], (LAYERS, HEADS), ((1, 4),), -0.2, 0.2), 0.5, 2.0),
        "conv_taps": scatter_about(key_of[10], (LAYERS, CONV, 3, SSD_DIM), CONV ** -0.5, 2.5, ((3, 4),)),
        "gate_gain": jnp.clip(1.0 + 0.18 * jax.random.normal(key_of[11], (LAYERS, SSD_DIM), jnp.float32), 0.1, 1.9),
        "w_project": scatter_about(key_of[12], (LAYERS, SSD_DIM, D), SSD_DIM ** -0.5, 0.109375, ((1, 4), (2, 8))),
        "states": scatter_about(key_of[13], (LAYERS, BATCH, HEADS, HEAD_DIM * STATE), 0.5, 3.0, ((1, 8), (2, 4)), jnp.float32),
        "recent": scatter_about(key_of[14], (LAYERS, BATCH, CONV - 1, 3, SSD_DIM), 1.0, 6.0, ((1, 8), (4, 4))),
    }


EPS = 1e-06

def run_block(tokens_now, level, norm_gain, w_gate, w_value, w_inmap, w_readout, w_step, step_bias, decay_log, skip_gain, conv_taps, gate_gain, w_project, states, recent):
    tokens_f = tokens_now.astype(jnp.float32)
    scale_one = lax.rsqrt(lax.optimization_barrier(jnp.mean(tokens_f * tokens_f, axis=-1, keepdims=True)) + EPS)
    gained = (tokens_f * norm_gain[level][None, :]).astype(jnp.bfloat16)

    def project(weight):
        return scale_one * jnp.dot(gained, weight[level], preferred_element_type=jnp.float32)
    gate_pre = project(w_gate)
    step_raw = project(w_step)
    stacked = jnp.stack([project(w_value), project(w_inmap), project(w_readout)], axis=1).astype(jnp.bfloat16)
    window = jnp.concatenate([recent[level], stacked[:, None]], axis=1)
    taps_sum = lax.optimization_barrier(jnp.sum(window.astype(jnp.float32) * conv_taps[level].astype(jnp.float32)[None], axis=1))
    active = jax.nn.silu(taps_sum)
    rows = tokens_now.shape[0]
    x_value = active[:, 0].reshape(rows, HEADS, HEAD_DIM)
    in_map = active[:, 1].reshape(rows, HEADS, STATE)
    out_map = active[:, 2].reshape(rows, HEADS, STATE)
    step_size = jax.nn.softplus(step_raw + step_bias[level][None, :])
    decay_rate = jnp.exp(-step_size * jnp.exp(decay_log[level])[None, :])
    old_state = states[level].reshape(rows, HEADS, HEAD_DIM, STATE)
    fresh = decay_rate[:, :, None, None] * old_state + (step_size[:, :, None] * x_value)[:, :, :, None] * in_map[:, :, None, :]
    head_out = jnp.einsum('bhpn,bhn->bhp', fresh, out_map) + skip_gain[level][None, :, None] * x_value
    gated = (head_out.reshape(rows, SSD_DIM) * jax.nn.silu(gate_pre) * gate_gain[level][None, :]).astype(jnp.bfloat16)
    gated_f = gated.astype(jnp.float32)
    scale_two = lax.rsqrt(lax.optimization_barrier(jnp.mean(gated_f * gated_f, axis=-1, keepdims=True)) + EPS)
    mixed_out = scale_two * jnp.dot(gated, w_project[level], preferred_element_type=jnp.float32)
    return ((tokens_f + mixed_out).astype(jnp.bfloat16), fresh.reshape(rows, HEADS, HEAD_DIM * STATE), window[:, 1:])

def reference(tokens, norm_gain, w_gate, w_value, w_inmap, w_readout, w_step, step_bias, decay_log, skip_gain, conv_taps, gate_gain, w_project, states, recent):
    current = tokens
    state_list = []
    recent_list = []
    for level in range(LAYERS):
        current, fresh, kept = run_block(current, level, norm_gain, w_gate, w_value, w_inmap, w_readout, w_step, step_bias, decay_log, skip_gain, conv_taps, gate_gain, w_project, states, recent)
        state_list.append(fresh)
        recent_list.append(kept)
    return (current, jnp.stack(state_list, axis=0), jnp.stack(recent_list, axis=0))
```

```python
import functools

import jax
import jax.numpy as jnp
from jax import lax
from jax.experimental import pallas as pl
from jax.experimental.pallas import tpu as pltpu
from jax.sharding import PartitionSpec as P

EPS = 1e-06
LANES = 128
MESH = pl.DeviceIdType.MESH
F32 = jnp.float32
BF16 = jnp.bfloat16
VMEM_BYTES = 67043328
READOUT, INMAP, VALUE, GATE = range(4)


def each(count, body, first=0):
    if count - first <= 8:
        for index in range(first, count):
            body(index)
    else:
        lax.fori_loop(first, count, lambda index, carry: (body(index), carry)[1], 0)


def fold(count, body, start, first=0):
    if count - first <= 8:
        for index in range(first, count):
            start = body(index, start)
        return start
    return lax.fori_loop(first, count, body, start)


def silu(value):
    return value / (1.0 + jnp.exp(-value))


def halves(value):
    high = value.astype(BF16)
    return high, (value - high.astype(F32)).astype(BF16)


def kernel(
    dims,
    tokens_hbm,
    norm_hbm,
    bias_hbm,
    rate_hbm,
    skip_hbm,
    gain_hbm,
    taps_hbm,
    recent_hbm,
    readout_hbm,
    inmap_hbm,
    value_hbm,
    gate_hbm,
    step_hbm,
    project_hbm,
    states_hbm,
    tokens_out,
    fresh_out,
    recent_out,
    tokens_ref,
    norm_ref,
    bias_ref,
    rate_ref,
    skip_ref,
    gain_ref,
    taps_ref,
    recent_ref,
    w_in,
    w_step,
    w_out,
    state,
    spread,
    gather,
    part_send,
    part_recv,
    extra_send,
    extra_recv,
    gated_all,
    mixed_all,
    square_all,
    conv_ref,
    params_ref,
    chosen_ref,
    dec_ref,
    bm_ref,
    cm_ref,
    wide_ref,
    x_ref,
    small_sem,
    in_sem,
    step_sem,
    out_sem,
    state_sem,
    send_sem,
    extra_sem,
    part_sem,
    gated_sem,
    mixed_sem,
    square_sem,
):
    layers, groups, dp, tp, own, cols, heads, head_dim, span, features, width = dims
    me = lax.axis_index("dp")
    col = lax.axis_index("tp")
    members = dp // groups
    rows = members * own
    mine = me // members
    place = lax.rem(me, members)

    def source(k):
        return lax.rem(me + k, dp)

    def member(g, k):
        return g * members + lax.rem(place + k, members)

    def column(k):
        return lax.rem(col + k + 1, tp)

    small = [
        pltpu.make_async_copy(far, near, small_sem.at[index])
        for index, (far, near) in enumerate((
            (tokens_hbm, tokens_ref),
            (norm_hbm, norm_ref),
            (bias_hbm, bias_ref),
            (rate_hbm, rate_ref),
            (skip_hbm, skip_ref),
            (gain_hbm, gain_ref),
            (taps_hbm, taps_ref),
            (recent_hbm, recent_ref),
        ))
    ]
    sources = (readout_hbm, inmap_hbm, value_hbm, gate_hbm)
    filled = step_hbm.shape[1]

    def load_step(level):
        return pltpu.make_async_copy(
            step_hbm.at[level], w_step.at[level, :filled], step_sem.at[level])

    def load_in(level, w):
        return pltpu.make_async_copy(
            sources[w].at[level], w_in.at[level, w], in_sem.at[level, w])

    def load_out(level):
        return pltpu.make_async_copy(project_hbm.at[level], w_out.at[level], out_sem.at[level])

    def load_state(level):
        return pltpu.make_async_copy(states_hbm.at[level], state.at[level], state_sem.at[level])

    for copy in small:
        copy.start()
    load_step(0).start()
    for w in range(4):
        load_in(0, w).start()

    barrier = pltpu.get_barrier_semaphore()
    each(dp, lambda k: pl.semaphore_signal(
        barrier, inc=1, device_id={"dp": source(k)}, device_id_type=MESH), 1)
    each(tp - 1, lambda k: pl.semaphore_signal(
        barrier, inc=1, device_id={"tp": column(k)}, device_id_type=MESH))

    def slot(target, origin):
        return lax.rem(origin - target + dp, dp) - 1

    def send_extra(level, target, origin):
        return pltpu.make_async_remote_copy(
            src_ref=extra_send.at[level, target],
            dst_ref=extra_recv.at[level, slot(target, origin)],
            send_sem=send_sem.at[0],
            recv_sem=extra_sem.at[level],
            device_id={"dp": target},
            device_id_type=MESH,
        )

    def send_part(level, w, target, origin):
        return pltpu.make_async_remote_copy(
            src_ref=part_send.at[level, w, target],
            dst_ref=part_recv.at[level, w, slot(target, origin)],
            send_sem=send_sem.at[1],
            recv_sem=part_sem.at[level, w],
            device_id={"dp": target},
            device_id_type=MESH,
        )

    def send_gated(level, target, origin):
        return pltpu.make_async_remote_copy(
            src_ref=gated_all.at[level, origin],
            dst_ref=gated_all.at[level, origin],
            send_sem=send_sem.at[2],
            recv_sem=gated_sem.at[level, mine],
            device_id={"dp": target},
            device_id_type=MESH,
        )

    def send_mixed(level, g, target, origin):
        return pltpu.make_async_remote_copy(
            src_ref=mixed_all.at[level, g, origin],
            dst_ref=mixed_all.at[level, g, origin],
            send_sem=send_sem.at[3],
            recv_sem=mixed_sem.at[level, g],
            device_id={"tp": target},
            device_id_type=MESH,
        )

    def send_square(level, g, target, origin):
        return pltpu.make_async_remote_copy(
            src_ref=square_all.at[level, g, origin],
            dst_ref=square_all.at[level, g, origin],
            send_sem=send_sem.at[4],
            recv_sem=square_sem.at[level, g],
            device_id={"tp": target},
            device_id_type=MESH,
        )

    def arrived(ref, sem):
        pltpu.make_async_remote_copy(
            src_ref=ref,
            dst_ref=ref,
            send_sem=send_sem.at[0],
            recv_sem=sem,
            device_id={"dp": source(1)},
            device_id_type=MESH,
        ).wait_recv()

    def sent(ref, index):
        pltpu.make_async_remote_copy(
            src_ref=ref,
            dst_ref=ref,
            send_sem=send_sem.at[index],
            recv_sem=extra_sem.at[0],
            device_id={"dp": source(1)},
            device_id_type=MESH,
        ).wait_send()

    def others(g, body):
        each(members, lambda k: body(member(g, k)), 1)
        if groups > 1:
            pl.when(mine != g)(lambda: body(member(g, 0)))

    low = lax.broadcasted_iota(jnp.int32, (own, LANES), 1) < head_dim

    def twice(pair, odd):
        turned = pltpu.roll(pair, head_dim, 1)
        return jnp.where(low, turned, pair) if odd else jnp.where(low, pair, turned)

    def project_in(level, first, count):
        span_rows = slice(first * rows, (first + count) * rows)
        span_devices = slice(first * members, (first + count) * members)
        x = x_ref[span_rows]
        square = jnp.sum(x * x, axis=1, keepdims=True)
        gained = (x * norm_ref[level][None, :]).astype(BF16)
        lane = lax.broadcasted_iota(jnp.int32, (count * rows, LANES), 1)
        load_step(level).wait() if first == 0 else None
        extra = lax.dot_general(
            gained, w_step[level], (((1,), (1,)), ((), ())), preferred_element_type=F32)
        extra = jnp.where(lane == LANES - 1, square, extra).reshape(count * members, own, LANES)
        high, rest = halves(extra)
        extra_send[level, span_devices, :, :LANES] = high
        extra_send[level, span_devices, :, LANES:] = rest
        if level == 0 and first == 0:
            pl.semaphore_wait(barrier, dp - 1 + tp - 1)
        others(first, lambda target: send_extra(level, target, me).start())
        for w in range(4):
            if first == 0:
                with jax.named_scope(f"w_in{w}_{level}"):
                    load_in(level, w).wait()
            part = jnp.dot(gained, w_in[level, w], preferred_element_type=F32)
            part_send[level, w, span_devices] = part.reshape(
                count * members, own, cols).astype(BF16)
            with jax.named_scope(f"send{w}_{level}_{first}"):
                others(first, lambda target: send_part(level, w, target, me).start())
        for g in range(first + 1, first + count):
            others(g, lambda target: send_extra(level, target, me).start())
            for w in range(4):
                others(g, lambda target: send_part(level, w, target, me).start())

    def prepare():
        w_step[:, filled:] = jnp.zeros((layers, LANES - filled, width), BF16)

    def build():
        step = 256
        which = lax.broadcasted_iota(jnp.int32, (LANES, step), 0)
        entry = lax.broadcasted_iota(jnp.int32, (LANES, step), 1)
        across_lanes = lax.rem(which, head_dim) - entry // span
        which = lax.broadcasted_iota(jnp.int32, (step, LANES), 1)
        entry = lax.broadcasted_iota(jnp.int32, (step, LANES), 0)
        along_rows = lax.rem(which, head_dim) - entry // span

        def fill(index, carry):
            start = pl.multiple_of(index * step, step)
            target = index * (step // span)
            spread[:, pl.ds(start, step)] = jnp.where(
                across_lanes == target, 1.0, 0.0).astype(BF16)
            gather[pl.ds(start, step), :] = jnp.where(
                along_rows == target, 1.0, 0.0).astype(BF16)
            return carry

        lax.fori_loop(0, head_dim * span // step, fill, 0)
        pick = lax.broadcasted_iota(jnp.int32, (LANES, cols), 0)
        slot = lax.broadcasted_iota(jnp.int32, (LANES, cols), 1)
        chosen_ref[...] = jnp.where(
            pick == col * heads + slot // head_dim, 1.0, 0.0).astype(BF16)
        pick = lax.broadcasted_iota(jnp.int32, (heads, cols), 0)
        slot = lax.broadcasted_iota(jnp.int32, (heads, cols), 1)
        wider = jnp.where(pick == slot // head_dim, 1.0, 0.0)
        for where, value in enumerate((bias_ref[...], jnp.exp(rate_ref[...]), skip_ref[...])):
            params_ref[where] = jnp.dot(
                value, wider, preferred_element_type=F32, precision=lax.Precision.HIGHEST)

    def convolve(level):
        for j in range(3):
            conv_ref[level, j] = jnp.sum(
                recent_ref[level, :, j].astype(F32)
                * taps_ref[: taps_ref.shape[0] - 1, j, level, :].astype(F32)[None],
                axis=1,
            )

    piece = 1024
    pieces = head_dim * span // piece

    def across(ref, h):
        return jnp.concatenate([ref[h]] * (piece // LANES), axis=1)

    def mix(level):
        with jax.named_scope(f"wr_extra_{level}"):
            arrived(extra_recv.at[level], extra_sem.at[level])
        both = fold(
            dp - 1,
            lambda k, sum_in: sum_in + extra_recv[level, k].astype(F32),
            extra_send[level, me].astype(F32),
        )
        total = both[:, :LANES] + both[:, LANES:]
        scale = lax.rsqrt(total[:, LANES - 1 :] / features + EPS)
        chosen = chosen_ref[...]
        high, rest = halves(total * scale)
        raw = jnp.dot(high, chosen, preferred_element_type=F32) + jnp.dot(
            rest, chosen, preferred_element_type=F32)
        raw = raw + params_ref[0, level : level + 1, :]
        size = jnp.maximum(raw, 0.0) + jnp.log1p(jnp.exp(-jnp.abs(raw)))
        decay = jnp.exp(-size * params_ref[1, level : level + 1, :])

        def total_part(w):
            with jax.named_scope(f"wr_part{w}_{level}"):
                arrived(part_recv.at[level, w], part_sem.at[level, w])
            return scale * fold(
                dp - 1,
                lambda k, sum_in: sum_in + part_recv[level, w, k].astype(F32),
                part_send[level, w, me].astype(F32),
            )

        fresh_u = {}

        def active(w, j):
            u = total_part(w).astype(BF16).astype(F32)
            fresh_u[j] = u
            return silu(
                conv_ref[level, j]
                + u * taps_ref[taps_ref.shape[0] - 1, j, level : level + 1, :].astype(F32))

        cm = active(READOUT, 2)
        for h in range(heads):
            window = slice(h // 2 * LANES, h // 2 * LANES + LANES)
            cm_ref[h] = twice(cm[:, window], h % 2)
        with jax.named_scope(f"w_state_{level}"):
            load_state(level).wait()
        y = jnp.zeros((heads * own, LANES), F32)
        with jax.named_scope(f"consult_{level}"):
            for index in range(pieces):
                window = slice(index * piece, index * piece + piece)
                read = jnp.concatenate(
                    [state[level, h, :, window] * across(cm_ref, h) for h in range(heads)], axis=0)
                y = y + jnp.dot(
                    read.astype(BF16), gather[window, :], preferred_element_type=F32)
        bm = active(INMAP, 1)
        for h in range(heads):
            window = slice(h // 2 * LANES, h // 2 * LANES + LANES)
            dec_ref[h] = twice(decay[:, window], h % 2)
            bm_ref[h] = twice(bm[:, window], h % 2)
        xv = active(VALUE, 0)
        weighted = size * xv
        inner = []
        for h in range(heads):
            window = slice(h // 2 * LANES, h // 2 * LANES + LANES)
            one = twice(weighted[:, window], h % 2)
            high = one.astype(BF16).astype(F32)
            wide_ref[h * own : (h + 1) * own, :] = jnp.where(low, high, one - high)
            within = jnp.sum(
                jnp.where(low, bm_ref[h] * cm_ref[h], 0.0), axis=1, keepdims=True)
            inner.append(dec_ref[h] * y[h * own : (h + 1) * own] + one * within)
        y = jnp.concatenate(
            [jnp.where(low, inner[h], inner[h + 1]) for h in range(0, heads, 2)], axis=1)
        y = (y + params_ref[2, level : level + 1, :] * xv) * gain_ref[level : level + 1, :]
        gate = total_part(GATE)
        gated_all[level, me] = (y * silu(gate)).astype(BF16)
        with jax.named_scope(f"s_gated_{level}"):
            each(dp, lambda k: send_gated(level, source(k), me).start(), 1)
        with jax.named_scope(f"advance_{level}"):
            wide = wide_ref[...].astype(BF16)

            def advance(index, carry):
                window = pl.ds(pl.multiple_of(index * piece, piece), piece)
                grown = jnp.dot(wide, spread[:, window], preferred_element_type=F32)
                for h in range(heads):
                    fresh_out[level, h, :, window] = (
                        across(dec_ref, h) * state[level, h, :, window]
                        + grown[h * own : (h + 1) * own] * across(bm_ref, h))
                return carry

            lax.fori_loop(0, pieces, advance, 0)
        with jax.named_scope(f"recent_{level}"):
            for j in range(3):
                kept = recent_ref[level, :, j].astype(F32)
                recent_out[level, :, j] = jnp.concatenate(
                    [kept[:, 1:], fresh_u[j][:, None]], axis=1).astype(BF16)

    cross = lax.broadcasted_iota(jnp.int32, (rows, rows), 0) == (
        lax.broadcasted_iota(jnp.int32, (rows, rows), 1))

    def project_out(level, g):
        if g == 0:
            load_out(level).wait()
        with jax.named_scope(f"wr_gated_{level}_{g}"):
            sem = gated_sem.at[level, g]
            if groups > 1:
                pl.when(mine == g)(lambda: arrived(gated_all.at[level, : members - 1], sem))
                pl.when(mine != g)(lambda: arrived(gated_all.at[level, :members], sem))
            else:
                arrived(gated_all.at[level, : members - 1], sem)
        gated = gated_all[level, g * members : (g + 1) * members].astype(F32).reshape(rows, cols)
        square = jnp.sum(gated * gated, axis=1, keepdims=True)
        square_all[level, g, col, :, :rows] = jnp.sum(
            jnp.where(cross, square, 0.0), axis=0, keepdims=True)
        each(tp - 1, lambda k: send_square(level, g, column(k), col).start())
        mixed = jnp.dot(gated.astype(BF16), w_out[level], preferred_element_type=F32)
        mixed_all[level, g, col] = mixed.astype(BF16)
        with jax.named_scope(f"s_mixed_{level}_{g}"):
            each(tp - 1, lambda k: send_mixed(level, g, column(k), col).start())

    def renew(level, g):
        arrived(square_all.at[level, g, : tp - 1], square_sem.at[level, g])
        square = fold(
            tp,
            lambda k, sum_in: sum_in + square_all[level, g, k, :, :rows],
            jnp.zeros((1, rows), F32),
        )
        scale = lax.rsqrt(square / (cols * tp) + EPS)
        scale = jnp.sum(jnp.where(cross, scale, 0.0), axis=1, keepdims=True)
        with jax.named_scope(f"wr_mixed_{level}_{g}"):
            arrived(mixed_all.at[level, g, : tp - 1], mixed_sem.at[level, g])
        mixed = fold(
            tp,
            lambda k, sum_in: sum_in + mixed_all[level, g, k].astype(F32),
            jnp.zeros((rows, width), F32),
        )
        window = slice(g * rows, (g + 1) * rows)
        fresh_x = (x_ref[window] + scale * mixed).astype(BF16)
        if level == layers - 1:
            tokens_out[window] = fresh_x
        else:
            x_ref[window] = fresh_x.astype(F32)

    prepare()
    small[0].wait()
    small[1].wait()
    x_ref[...] = tokens_ref[...].astype(F32)
    project_in(0, 0, groups)
    load_state(0).start()
    load_out(0).start()
    for level in range(1, layers):
        load_step(level).start()
        for w in range(4):
            load_in(level, w).start()
        load_state(level).start()
        load_out(level).start()
    with jax.named_scope("small_wait"):
        for copy in small[2:]:
            copy.wait()
    with jax.named_scope("build"):
        build()
        for level in range(layers):
            convolve(level)
    for level in range(layers):
        mix(level)
        for g in range(groups):
            project_out(level, g)
        for g in range(groups):
            renew(level, g)
            if level < layers - 1:
                project_in(level + 1, g, 1)

    sent(extra_recv, 0)
    sent(part_recv, 1)
    sent(part_recv.at[:, 0], 2)
    sent(mixed_all.at[:, :, : tp - 1], 3)
    sent(square_all.at[:, :, : tp - 1], 4)


def finish(tokens_ref, fresh_ref, recent_ref, tokens_hbm, fresh_hbm, recent_hbm, sem):
    layers, heads = fresh_ref.shape[:2]
    for level in range(layers):
        for h in range(heads):
            pltpu.make_async_copy(
                fresh_ref.at[level, h], fresh_hbm.at[level, h], sem.at[0]).start()
    small = (
        pltpu.make_async_copy(tokens_ref, tokens_hbm, sem.at[1]),
        pltpu.make_async_copy(recent_ref, recent_hbm, sem.at[2]),
    )
    for copy in small:
        copy.start()
    for copy in small:
        copy.wait()
    pltpu.make_async_copy(fresh_ref, fresh_hbm, sem.at[0]).wait()


def per_device(
    dp,
    tp,
    tokens,
    norm_gain,
    w_gate,
    w_value,
    w_inmap,
    w_readout,
    w_step,
    step_bias,
    decay_log,
    skip_gain,
    conv_taps,
    gate_gain,
    w_project,
    states,
    recent,
):
    layers, own, heads, entries = states.shape
    cols = w_gate.shape[2]
    head_dim = cols // heads
    span = entries // head_dim
    width = tokens.shape[1]
    features = width * dp
    groups = GROUPS if dp % GROUPS == 0 else 1
    dims = (layers, groups, dp, tp, own, cols, heads, head_dim, span, features, width)
    total = tokens.shape[0]
    rows = total // groups

    vmem = pl.BlockSpec(memory_space=pltpu.VMEM)
    anywhere = pl.BlockSpec(memory_space=pltpu.HBM)
    turned = recent.transpose(0, 1, 3, 2, 4)
    taps = conv_taps.transpose(1, 2, 0, 3)
    dma = pltpu.SemaphoreType.DMA
    padded = -(-rows // LANES) * LANES
    kept_bytes = 2 * tokens.size + 4 * states.size + 2 * recent.size
    results = pl.pallas_call(
        functools.partial(kernel, dims),
        out_shape=(
            pltpu.VMEM((total, width), BF16),
            pltpu.VMEM((layers, heads, own, entries), F32),
            pltpu.VMEM(turned.shape, BF16),
        ),
        in_specs=[anywhere] * 15,
        out_specs=(vmem, vmem, vmem),
        scratch_shapes=[
            pltpu.VMEM(tokens.shape, BF16),
            pltpu.VMEM(norm_gain.shape, F32),
            pltpu.VMEM(step_bias.shape, F32),
            pltpu.VMEM(decay_log.shape, F32),
            pltpu.VMEM(skip_gain.shape, F32),
            pltpu.VMEM(gate_gain.shape, F32),
            pltpu.VMEM(taps.shape, BF16),
            pltpu.VMEM(turned.shape, BF16),
            pltpu.VMEM((layers, 4, width, cols), BF16),
            pltpu.VMEM((layers, LANES, width), BF16),
            pltpu.VMEM((layers, cols, width), BF16),
            pltpu.VMEM((layers, heads, own, entries), F32),
            pltpu.VMEM((LANES, entries), BF16),
            pltpu.VMEM((entries, LANES), BF16),
            pltpu.VMEM((layers, 4, dp, own, cols), BF16),
            pltpu.VMEM((layers, 4, dp - 1, own, cols), BF16),
            pltpu.VMEM((layers, dp, own, 2 * LANES), BF16),
            pltpu.VMEM((layers, dp - 1, own, 2 * LANES), BF16),
            pltpu.VMEM((layers, dp, own, cols), BF16),
            pltpu.VMEM((layers, groups, tp, rows, width), BF16),
            pltpu.VMEM((layers, groups, tp, 1, padded), F32),
            pltpu.VMEM((layers, 3, own, cols), F32),
            pltpu.VMEM((3, layers, cols), F32),
            pltpu.VMEM((LANES, cols), BF16),
            pltpu.VMEM((heads, own, LANES), F32),
            pltpu.VMEM((heads, own, LANES), F32),
            pltpu.VMEM((heads, own, LANES), F32),
            pltpu.VMEM((heads * own, LANES), F32),
            pltpu.VMEM((total, width), F32),
            dma((8,)),
            dma((layers, 4)),
            dma((layers,)),
            dma((layers,)),
            dma((layers,)),
            dma((5,)),
            dma((layers,)),
            dma((layers, 4)),
            dma((layers, groups)),
            dma((layers, groups)),
            dma((layers, groups)),
        ],
        compiler_params=pltpu.CompilerParams(
            collective_id=0, has_side_effects=True, vmem_limit_bytes=VMEM_BYTES - kept_bytes),
    )(
        tokens,
        norm_gain,
        step_bias,
        decay_log,
        skip_gain,
        gate_gain,
        taps,
        turned,
        w_readout,
        w_inmap,
        w_value,
        w_gate,
        w_step.transpose(0, 2, 1),
        w_project,
        states.transpose(0, 2, 1, 3),
    )
    out_tokens, fresh, kept = pl.pallas_call(
        finish,
        out_shape=(
            jax.ShapeDtypeStruct((total, width), BF16),
            jax.ShapeDtypeStruct((layers, heads, own, entries), F32),
            jax.ShapeDtypeStruct(turned.shape, BF16),
        ),
        in_specs=[vmem] * 3,
        out_specs=(anywhere,) * 3,
        scratch_shapes=[dma((3,))],
        compiler_params=pltpu.CompilerParams(vmem_limit_bytes=16 * 1024 * 1024),
    )(*results)
    next_states = fresh.transpose(0, 2, 1, 3)
    next_recent = kept.transpose(0, 1, 3, 2, 4)
    return out_tokens, next_states, next_recent


GROUPS = 2
def solution(mesh):
    in_specs = (
        P(None, "dp"),
        P(None, "dp"),
        P(None, "dp", "tp"),
        P(None, "dp", "tp"),
        P(None, "dp", "tp"),
        P(None, "dp", "tp"),
        P(None, "dp", None),
        P(None, "tp"),
        P(None, "tp"),
        P(None, "tp"),
        P(None, None, None, "tp"),
        P(None, "tp"),
        P(None, "tp", "dp"),
        P(None, "dp", "tp", None),
        P(None, "dp", None, None, "tp"),
    )
    out_specs = (P(None, "dp"), P(None, "dp", "tp", None), P(None, "dp", None, None, "tp"))
    body = functools.partial(per_device, mesh.shape["dp"], mesh.shape["tp"])
    return jax.shard_map(
        body, mesh=mesh, in_specs=in_specs, out_specs=out_specs, check_vma=False
    )
```

```python
import functools

import jax
import jax.numpy as jnp
from jax import lax
from jax.experimental import pallas as pl
from jax.experimental.pallas import tpu as pltpu
from jax.sharding import PartitionSpec as P

EPS = 1e-06
LANES = 128
MESH = pl.DeviceIdType.MESH
F32 = jnp.float32
BF16 = jnp.bfloat16
VMEM_BYTES = 67043328
READOUT, INMAP, VALUE, GATE = range(4)


def each(count, body, first=0):
    if count - first <= 8:
        for index in range(first, count):
            body(index)
    else:
        lax.fori_loop(first, count, lambda index, carry: (body(index), carry)[1], 0)


def fold(count, body, start, first=0):
    if count - first <= 8:
        for index in range(first, count):
            start = body(index, start)
        return start
    return lax.fori_loop(first, count, body, start)


def silu(value):
    return value / (1.0 + jnp.exp(-value))


def halves(value):
    high = value.astype(BF16)
    return high, (value - high.astype(F32)).astype(BF16)


def kernel(
    dims,
    tokens_hbm,
    norm_hbm,
    bias_hbm,
    rate_hbm,
    skip_hbm,
    gain_hbm,
    taps_hbm,
    recent_hbm,
    readout_hbm,
    inmap_hbm,
    value_hbm,
    gate_hbm,
    step_hbm,
    project_hbm,
    states_hbm,
    tokens_out,
    fresh_out,
    recent_out,
    tokens_ref,
    norm_ref,
    bias_ref,
    rate_ref,
    skip_ref,
    gain_ref,
    taps_ref,
    recent_ref,
    w_in,
    w_step,
    w_out,
    state,
    spread,
    gather,
    part_send,
    part_recv,
    extra_send,
    extra_recv,
    gated_all,
    mixed_all,
    square_all,
    conv_ref,
    params_ref,
    chosen_ref,
    dec_ref,
    bm_ref,
    cm_ref,
    wide_ref,
    x_ref,
    small_sem,
    in_sem,
    step_sem,
    out_sem,
    state_sem,
    send_sem,
    extra_sem,
    part_sem,
    gated_sem,
    mixed_sem,
    square_sem,
):
    layers, groups, dp, tp, own, cols, heads, head_dim, span, features, width = dims
    me = lax.axis_index("dp")
    col = lax.axis_index("tp")
    members = dp // groups
    rows = members * own
    mine = lax.rem(me, groups)
    place = me // groups

    def moved(k):
        if members & (members - 1):
            return lax.rem(place + k, members)
        return sum(
            lax.rem(place // bit + k // bit, 2) * bit
            for bit in (1 << power for power in range(members.bit_length() - 1)))

    def member(g, k):
        return moved(k) * groups + g

    def slot(g, k):
        return k * groups + lax.rem(g - mine + groups, groups) - 1

    def column(k):
        return lax.rem(col + k + 1, tp)

    def columns(body):
        def at(index):
            pl.when(col + tp - index < tp)(lambda: body(col + tp - index))
            pl.when(col + index >= tp)(lambda: body(col + index - tp))

        each(tp, at, 1)

    small = [
        pltpu.make_async_copy(far, near, small_sem.at[index])
        for index, (far, near) in enumerate((
            (tokens_hbm, tokens_ref),
            (norm_hbm, norm_ref),
            (bias_hbm, bias_ref),
            (rate_hbm, rate_ref),
            (skip_hbm, skip_ref),
            (gain_hbm, gain_ref),
            (taps_hbm, taps_ref),
            (recent_hbm, recent_ref),
        ))
    ]
    sources = (readout_hbm, inmap_hbm, value_hbm, gate_hbm)
    filled = step_hbm.shape[1]

    def load_step(level):
        return pltpu.make_async_copy(
            step_hbm.at[level], w_step.at[level, :filled], step_sem.at[level])

    def load_in(level, w):
        return pltpu.make_async_copy(
            sources[w].at[level], w_in.at[level, w], in_sem.at[level, w])

    def load_out(level):
        return pltpu.make_async_copy(project_hbm.at[level], w_out.at[level], out_sem.at[level])

    def load_state(level):
        return pltpu.make_async_copy(states_hbm.at[level], state.at[level], state_sem.at[level])

    for copy in small[:2]:
        copy.start()
    load_step(0).start()
    load_in(0, 0).start()
    load_in(0, 1).start()

    barrier = pltpu.get_barrier_semaphore()
    each(dp, lambda k: pl.semaphore_signal(
        barrier, inc=1, device_id={"dp": lax.rem(me + k, dp)}, device_id_type=MESH), 1)
    each(tp - 1, lambda k: pl.semaphore_signal(
        barrier, inc=1, device_id={"tp": column(k)}, device_id_type=MESH))

    def send_extra(level, g, k):
        return pltpu.make_async_remote_copy(
            src_ref=extra_send.at[level, g, moved(k)],
            dst_ref=extra_recv.at[level, slot(g, k)],
            send_sem=send_sem.at[0],
            recv_sem=extra_sem.at[level],
            device_id={"dp": member(g, k)},
            device_id_type=MESH,
        )

    def send_part(level, w, g, k):
        return pltpu.make_async_remote_copy(
            src_ref=part_send.at[level, w, g, moved(k)],
            dst_ref=part_recv.at[level, w, slot(g, k)],
            send_sem=send_sem.at[1],
            recv_sem=part_sem.at[level, w],
            device_id={"dp": member(g, k)},
            device_id_type=MESH,
        )

    def send_gated(level, g, k):
        return pltpu.make_async_remote_copy(
            src_ref=gated_all.at[level, mine, place],
            dst_ref=gated_all.at[level, mine, place],
            send_sem=send_sem.at[2],
            recv_sem=gated_sem.at[level, mine],
            device_id={"dp": member(g, k)},
            device_id_type=MESH,
        )

    def send_mixed(level, g, target, origin):
        return pltpu.make_async_remote_copy(
            src_ref=mixed_all.at[level, g, origin],
            dst_ref=mixed_all.at[level, g, origin],
            send_sem=send_sem.at[3],
            recv_sem=mixed_sem.at[level, g],
            device_id={"tp": target},
            device_id_type=MESH,
        )

    def send_square(level, g, target, origin):
        return pltpu.make_async_remote_copy(
            src_ref=square_all.at[level, g, origin],
            dst_ref=square_all.at[level, g, origin],
            send_sem=send_sem.at[4],
            recv_sem=square_sem.at[level, g],
            device_id={"tp": target},
            device_id_type=MESH,
        )

    def arrived(ref, sem):
        pltpu.make_async_remote_copy(
            src_ref=ref,
            dst_ref=ref,
            send_sem=send_sem.at[0],
            recv_sem=sem,
            device_id={"dp": lax.rem(me + 1, dp)},
            device_id_type=MESH,
        ).wait_recv()

    def sent(ref, index):
        pltpu.make_async_remote_copy(
            src_ref=ref,
            dst_ref=ref,
            send_sem=send_sem.at[index],
            recv_sem=extra_sem.at[0],
            device_id={"dp": lax.rem(me + 1, dp)},
            device_id_type=MESH,
        ).wait_send()

    def others(which, body):
        def far(index):
            for g in which:
                body(g, members - index)

        each(members, far, 1)
        for g in which:
            if groups > 1:
                pl.when(mine != g)(functools.partial(body, g, 0))

    def every(level, w, which):
        others(which, lambda g, k: send_part(level, w, g, k).start())

    low = lax.broadcasted_iota(jnp.int32, (own, LANES), 1) < head_dim

    def twice(pair, odd):
        turned = pltpu.roll(pair, head_dim, 1)
        return jnp.where(low, turned, pair) if odd else jnp.where(low, pair, turned)

    def project_in(level, first, count):
        x = x_ref[first : first + count].reshape(count * rows, width)
        square = jnp.sum(x * x, axis=1, keepdims=True)
        gained = (x * norm_ref[level][None, :]).astype(BF16)
        lane = lax.broadcasted_iota(jnp.int32, (count * rows, LANES), 1)

        def store(w):
            part = jnp.dot(gained, w_in[level, w], preferred_element_type=F32)
            part_send[level, w, first : first + count] = part.reshape(
                count, members, own, cols).astype(BF16)

        if first == 0:
            with jax.named_scope(f"w_step_{level}"):
                load_step(level).wait()
        extra = lax.dot_general(
            gained, w_step[level], (((1,), (1,)), ((), ())), preferred_element_type=F32)
        extra = jnp.where(lane == LANES - 1, square, extra).reshape(count, members, own, LANES)
        high, rest = halves(extra)
        if first == 0:
            with jax.named_scope(f"w_in0_{level}"):
                load_in(level, 0).wait()
        extra_send[level, first : first + count, :, :, :LANES] = high
        extra_send[level, first : first + count, :, :, LANES:] = rest
        store(0)
        if level == 0 and first == 0:
            with jax.named_scope("barrier"):
                pl.semaphore_wait(barrier, dp - 1 + tp - 1)
        which = range(first, first + count)
        others(which, lambda g, k: send_extra(level, g, k).start())
        every(level, 0, which[:1])
        for w in range(1, 4):
            if first == 0:
                with jax.named_scope(f"w_in{w}_{level}"):
                    load_in(level, w).wait()
            store(w)
            with jax.named_scope(f"send{w}_{level}_{first}"):
                every(level, w, which[:1])
        for w in range(4):
            if count > 1:
                every(level, w, which[1:])

    def prepare():
        w_step[:, filled:] = jnp.zeros((layers, LANES - filled, width), BF16)

    def build():
        step = 256
        which = lax.broadcasted_iota(jnp.int32, (LANES, step), 0)
        entry = lax.broadcasted_iota(jnp.int32, (LANES, step), 1)
        across_lanes = lax.rem(which, head_dim) - entry // span
        which = lax.broadcasted_iota(jnp.int32, (step, LANES), 1)
        entry = lax.broadcasted_iota(jnp.int32, (step, LANES), 0)
        along_rows = lax.rem(which, head_dim) - entry // span

        def fill(index, carry):
            start = pl.multiple_of(index * step, step)
            target = index * (step // span)
            spread[:, pl.ds(start, step)] = jnp.where(
                across_lanes == target, 1.0, 0.0).astype(BF16)
            gather[pl.ds(start, step), :] = jnp.where(
                along_rows == target, 1.0, 0.0).astype(BF16)
            return carry

        lax.fori_loop(0, head_dim * span // step, fill, 0)
        pick = lax.broadcasted_iota(jnp.int32, (LANES, cols), 0)
        slot = lax.broadcasted_iota(jnp.int32, (LANES, cols), 1)
        chosen_ref[...] = jnp.where(
            pick == col * heads + slot // head_dim, 1.0, 0.0).astype(BF16)
        pick = lax.broadcasted_iota(jnp.int32, (heads, cols), 0)
        slot = lax.broadcasted_iota(jnp.int32, (heads, cols), 1)
        wider = jnp.where(pick == slot // head_dim, 1.0, 0.0)
        for where, value in enumerate((bias_ref[...], jnp.exp(rate_ref[...]), skip_ref[...])):
            params_ref[where] = jnp.dot(
                value, wider, preferred_element_type=F32, precision=lax.Precision.HIGHEST)

    def convolve(level):
        for j in range(3):
            conv_ref[level, j] = jnp.sum(
                recent_ref[level, :, j].astype(F32)
                * taps_ref[: taps_ref.shape[0] - 1, j, level, :].astype(F32)[None],
                axis=1,
            )

    piece = 1024
    pieces = head_dim * span // piece

    def across(ref, h):
        return jnp.concatenate([ref[h]] * (piece // LANES), axis=1)

    def mix(level):
        with jax.named_scope(f"wr_extra_{level}"):
            arrived(extra_recv.at[level], extra_sem.at[level])
        both = fold(
            dp - 1,
            lambda k, sum_in: sum_in + extra_recv[level, k].astype(F32),
            extra_send[level, mine, place].astype(F32),
        )
        total = both[:, :LANES] + both[:, LANES:]
        scale = lax.rsqrt(total[:, LANES - 1 :] / features + EPS)
        def await_part(w):
            with jax.named_scope(f"wr_part{w}_{level}"):
                arrived(part_recv.at[level, w], part_sem.at[level, w])

        def total_part(w):
            return scale * fold(
                dp - 1,
                lambda k, sum_in: sum_in + part_recv[level, w, k].astype(F32),
                part_send[level, w, mine, place].astype(F32),
            )

        fresh_u = {}

        def active(w, j):
            u = total_part(w).astype(BF16).astype(F32)
            fresh_u[j] = u
            return silu(
                conv_ref[level, j]
                + u * taps_ref[taps_ref.shape[0] - 1, j, level : level + 1, :].astype(F32))

        load_state(level).wait()
        await_part(READOUT)
        cm = active(READOUT, 2)
        for h in range(heads):
            window = slice(h // 2 * LANES, h // 2 * LANES + LANES)
            cm_ref[h] = twice(cm[:, window], h % 2)
        y = jnp.zeros((heads * own, LANES), F32)
        for index in range(pieces):
            window = slice(index * piece, index * piece + piece)
            read = jnp.concatenate(
                [state[level, h, :, window] * across(cm_ref, h) for h in range(heads)], axis=0)
            y = y + jnp.dot(
                read.astype(BF16), gather[window, :], preferred_element_type=F32)
        chosen = chosen_ref[...]
        high, rest = halves(total * scale)
        raw = jnp.dot(high, chosen, preferred_element_type=F32) + jnp.dot(
            rest, chosen, preferred_element_type=F32)
        raw = raw + params_ref[0, level : level + 1, :]
        size = jnp.maximum(raw, 0.0) + jnp.log1p(jnp.exp(-jnp.abs(raw)))
        decay = jnp.exp(-size * params_ref[1, level : level + 1, :])

        await_part(INMAP)
        await_part(VALUE)
        bm = active(INMAP, 1)
        for h in range(heads):
            window = slice(h // 2 * LANES, h // 2 * LANES + LANES)
            dec_ref[h] = twice(decay[:, window], h % 2)
            bm_ref[h] = twice(bm[:, window], h % 2)
        xv = active(VALUE, 0)
        weighted = size * xv
        inner = []
        for h in range(heads):
            window = slice(h // 2 * LANES, h // 2 * LANES + LANES)
            one = twice(weighted[:, window], h % 2)
            high = one.astype(BF16).astype(F32)
            wide_ref[h * own : (h + 1) * own, :] = jnp.where(low, high, one - high)
            within = jnp.sum(
                jnp.where(low, bm_ref[h] * cm_ref[h], 0.0), axis=1, keepdims=True)
            inner.append(dec_ref[h] * y[h * own : (h + 1) * own] + one * within)
        y = jnp.concatenate(
            [jnp.where(low, inner[h], inner[h + 1]) for h in range(0, heads, 2)], axis=1)
        y = (y + params_ref[2, level : level + 1, :] * xv) * gain_ref[level : level + 1, :]
        await_part(GATE)
        gate = total_part(GATE)
        gated_all[level, mine, place] = (y * silu(gate)).astype(BF16)
        with jax.named_scope(f"s_gated_{level}"):
            others(range(groups), lambda g, k: send_gated(level, g, k).start())
        with jax.named_scope(f"advance_{level}"):
            wide = wide_ref[...].astype(BF16)

            def advance(index, carry):
                window = pl.ds(pl.multiple_of(index * piece, piece), piece)
                grown = jnp.dot(wide, spread[:, window], preferred_element_type=F32)
                for h in range(heads):
                    fresh_out[level, h, :, window] = (
                        across(dec_ref, h) * state[level, h, :, window]
                        + grown[h * own : (h + 1) * own] * across(bm_ref, h))
                return carry

            lax.fori_loop(0, pieces, advance, 0)
        with jax.named_scope(f"recent_{level}"):
            for j in range(3):
                kept = recent_ref[level, :, j].astype(F32)
                recent_out[level, :, j] = jnp.concatenate(
                    [kept[:, 1:], fresh_u[j][:, None]], axis=1).astype(BF16)

    cross = lax.broadcasted_iota(jnp.int32, (rows, rows), 0) == (
        lax.broadcasted_iota(jnp.int32, (rows, rows), 1))

    def project_out(level, g):
        if g == 0:
            load_out(level).wait()
        with jax.named_scope(f"wr_gated_{level}_{g}"):
            sem = gated_sem.at[level, g]
            if groups > 1:
                pl.when(mine == g)(lambda: arrived(gated_all.at[level, g, : members - 1], sem))
                pl.when(mine != g)(lambda: arrived(gated_all.at[level, g], sem))
            else:
                arrived(gated_all.at[level, g, : members - 1], sem)
        gated = gated_all[level, g].astype(F32).reshape(rows, cols)
        square = jnp.sum(gated * gated, axis=1, keepdims=True)
        square_all[level, g, col, :, :rows] = jnp.sum(
            jnp.where(cross, square, 0.0), axis=0, keepdims=True)
        columns(lambda target: send_square(level, g, target, col).start())
        mixed = jnp.dot(gated.astype(BF16), w_out[level], preferred_element_type=F32)
        mixed_all[level, g, col] = mixed.astype(BF16)
        with jax.named_scope(f"s_mixed_{level}_{g}"):
            columns(lambda target: send_mixed(level, g, target, col).start())

    def renew(level, g):
        arrived(square_all.at[level, g, : tp - 1], square_sem.at[level, g])
        square = fold(
            tp,
            lambda k, sum_in: sum_in + square_all[level, g, k, :, :rows],
            jnp.zeros((1, rows), F32),
        )
        scale = lax.rsqrt(square / (cols * tp) + EPS)
        scale = jnp.sum(jnp.where(cross, scale, 0.0), axis=1, keepdims=True)
        with jax.named_scope(f"wr_mixed_{level}_{g}"):
            arrived(mixed_all.at[level, g, : tp - 1], mixed_sem.at[level, g])
        mixed = fold(
            tp,
            lambda k, sum_in: sum_in + mixed_all[level, g, k].astype(F32),
            jnp.zeros((rows, width), F32),
        )
        fresh_x = (x_ref[g] + scale * mixed).astype(BF16)
        if level == layers - 1:
            for k in range(members):
                target = (k * groups + g) * own
                tokens_out[target : target + own] = fresh_x[k * own : (k + 1) * own]
        else:
            x_ref[g] = fresh_x.astype(F32)

    prepare()
    with jax.named_scope("tokens"):
        small[0].wait()
        small[1].wait()
    load_in(0, 2).start()
    load_in(0, 3).start()
    for copy in small[2:]:
        copy.start()
    x = tokens_ref[...].astype(F32).reshape(members, groups, own, width)
    for g in range(groups):
        x_ref[g] = x[:, g].reshape(rows, width)
    project_in(0, 0, groups)
    load_state(0).start()
    load_out(0).start()
    for level in range(1, layers):
        load_step(level).start()
        for w in range(4):
            load_in(level, w).start()
        load_state(level).start()
        load_out(level).start()
    with jax.named_scope("small_wait"):
        for copy in small[2:]:
            copy.wait()
    with jax.named_scope("build"):
        build()
        for level in range(layers):
            convolve(level)
    for level in range(layers):
        mix(level)
        for g in range(groups):
            project_out(level, g)
        for g in range(groups):
            renew(level, g)
            if level < layers - 1:
                project_in(level + 1, g, 1)

    sent(extra_recv, 0)
    sent(part_recv, 1)
    sent(part_recv.at[:, 0], 2)
    sent(mixed_all.at[:, :, : tp - 1], 3)
    sent(square_all.at[:, :, : tp - 1], 4)


def finish(tokens_ref, fresh_ref, recent_ref, tokens_hbm, fresh_hbm, recent_hbm, sem):
    layers, heads = fresh_ref.shape[:2]
    for level in range(layers):
        for h in range(heads):
            pltpu.make_async_copy(
                fresh_ref.at[level, h], fresh_hbm.at[level, h], sem.at[0]).start()
    small = (
        pltpu.make_async_copy(tokens_ref, tokens_hbm, sem.at[1]),
        pltpu.make_async_copy(recent_ref, recent_hbm, sem.at[2]),
    )
    for copy in small:
        copy.start()
    for copy in small:
        copy.wait()
    pltpu.make_async_copy(fresh_ref, fresh_hbm, sem.at[0]).wait()


def per_device(
    dp,
    tp,
    tokens,
    norm_gain,
    w_gate,
    w_value,
    w_inmap,
    w_readout,
    w_step,
    step_bias,
    decay_log,
    skip_gain,
    conv_taps,
    gate_gain,
    w_project,
    states,
    recent,
):
    layers, own, heads, entries = states.shape
    cols = w_gate.shape[2]
    head_dim = cols // heads
    span = entries // head_dim
    width = tokens.shape[1]
    features = width * dp
    groups = GROUPS if dp % GROUPS == 0 else 1
    dims = (layers, groups, dp, tp, own, cols, heads, head_dim, span, features, width)
    total = tokens.shape[0]
    rows = total // groups

    vmem = pl.BlockSpec(memory_space=pltpu.VMEM)
    anywhere = pl.BlockSpec(memory_space=pltpu.HBM)
    turned = recent.transpose(0, 1, 3, 2, 4)
    taps = conv_taps.transpose(1, 2, 0, 3)
    dma = pltpu.SemaphoreType.DMA
    padded = -(-rows // LANES) * LANES
    kept_bytes = 2 * tokens.size + 4 * states.size + 2 * recent.size
    results = pl.pallas_call(
        functools.partial(kernel, dims),
        out_shape=(
            pltpu.VMEM((total, width), BF16),
            pltpu.VMEM((layers, heads, own, entries), F32),
            pltpu.VMEM(turned.shape, BF16),
        ),
        in_specs=[anywhere] * 15,
        out_specs=(vmem, vmem, vmem),
        scratch_shapes=[
            pltpu.VMEM(tokens.shape, BF16),
            pltpu.VMEM(norm_gain.shape, F32),
            pltpu.VMEM(step_bias.shape, F32),
            pltpu.VMEM(decay_log.shape, F32),
            pltpu.VMEM(skip_gain.shape, F32),
            pltpu.VMEM(gate_gain.shape, F32),
            pltpu.VMEM(taps.shape, BF16),
            pltpu.VMEM(turned.shape, BF16),
            pltpu.VMEM((layers, 4, width, cols), BF16),
            pltpu.VMEM((layers, LANES, width), BF16),
            pltpu.VMEM((layers, cols, width), BF16),
            pltpu.VMEM((layers, heads, own, entries), F32),
            pltpu.VMEM((LANES, entries), BF16),
            pltpu.VMEM((entries, LANES), BF16),
            pltpu.VMEM((layers, 4, groups, dp // groups, own, cols), BF16),
            pltpu.VMEM((layers, 4, dp - 1, own, cols), BF16),
            pltpu.VMEM((layers, groups, dp // groups, own, 2 * LANES), BF16),
            pltpu.VMEM((layers, dp - 1, own, 2 * LANES), BF16),
            pltpu.VMEM((layers, groups, dp // groups, own, cols), BF16),
            pltpu.VMEM((layers, groups, tp, rows, width), BF16),
            pltpu.VMEM((layers, groups, tp, 1, padded), F32),
            pltpu.VMEM((layers, 3, own, cols), F32),
            pltpu.VMEM((3, layers, cols), F32),
            pltpu.VMEM((LANES, cols), BF16),
            pltpu.VMEM((heads, own, LANES), F32),
            pltpu.VMEM((heads, own, LANES), F32),
            pltpu.VMEM((heads, own, LANES), F32),
            pltpu.VMEM((heads * own, LANES), F32),
            pltpu.VMEM((groups, rows, width), F32),
            dma((8,)),
            dma((layers, 4)),
            dma((layers,)),
            dma((layers,)),
            dma((layers,)),
            dma((5,)),
            dma((layers,)),
            dma((layers, 4)),
            dma((layers, groups)),
            dma((layers, groups)),
            dma((layers, groups)),
        ],
        compiler_params=pltpu.CompilerParams(
            collective_id=0, has_side_effects=True, vmem_limit_bytes=VMEM_BYTES - kept_bytes),
    )(
        tokens,
        norm_gain,
        step_bias,
        decay_log,
        skip_gain,
        gate_gain,
        taps,
        turned,
        w_readout,
        w_inmap,
        w_value,
        w_gate,
        w_step.transpose(0, 2, 1),
        w_project,
        states.transpose(0, 2, 1, 3),
    )
    out_tokens, fresh, kept = pl.pallas_call(
        finish,
        out_shape=(
            jax.ShapeDtypeStruct((total, width), BF16),
            jax.ShapeDtypeStruct((layers, heads, own, entries), F32),
            jax.ShapeDtypeStruct(turned.shape, BF16),
        ),
        in_specs=[vmem] * 3,
        out_specs=(anywhere,) * 3,
        scratch_shapes=[dma((3,))],
        compiler_params=pltpu.CompilerParams(vmem_limit_bytes=16 * 1024 * 1024),
    )(*results)
    next_states = fresh.transpose(0, 2, 1, 3)
    next_recent = kept.transpose(0, 1, 3, 2, 4)
    return out_tokens, next_states, next_recent


GROUPS = 2
def solution(mesh):
    in_specs = (
        P(None, "dp"),
        P(None, "dp"),
        P(None, "dp", "tp"),
        P(None, "dp", "tp"),
        P(None, "dp", "tp"),
        P(None, "dp", "tp"),
        P(None, "dp", None),
        P(None, "tp"),
        P(None, "tp"),
        P(None, "tp"),
        P(None, None, None, "tp"),
        P(None, "tp"),
        P(None, "tp", "dp"),
        P(None, "dp", "tp", None),
        P(None, "dp", None, None, "tp"),
    )
    out_specs = (P(None, "dp"), P(None, "dp", "tp", None), P(None, "dp", None, None, "tp"))
    body = functools.partial(per_device, mesh.shape["dp"], mesh.shape["tp"])
    return jax.shard_map(
        body, mesh=mesh, in_specs=in_specs, out_specs=out_specs, check_vma=False
    )
```

```python
import functools

import jax
import jax.numpy as jnp
from jax import lax
from jax.experimental import pallas as pl
from jax.experimental.pallas import tpu as pltpu
from jax.sharding import PartitionSpec as P

EPS = 1e-06
LANES = 128
MESH = pl.DeviceIdType.MESH
F32 = jnp.float32
BF16 = jnp.bfloat16
VMEM_BYTES = 67043328
READOUT, INMAP, VALUE, GATE = range(4)


def each(count, body, first=0):
    if count - first <= 8:
        for index in range(first, count):
            body(index)
    else:
        lax.fori_loop(first, count, lambda index, carry: (body(index), carry)[1], 0)


def fold(count, body, start, first=0):
    if count - first <= 8:
        for index in range(first, count):
            start = body(index, start)
        return start
    return lax.fori_loop(first, count, body, start)


def silu(value):
    return value / (1.0 + jnp.exp(-value))


def halves(value):
    high = value.astype(BF16)
    return high, (value - high.astype(F32)).astype(BF16)


def kernel(
    dims,
    tokens_hbm,
    norm_hbm,
    bias_hbm,
    rate_hbm,
    skip_hbm,
    gain_hbm,
    taps_hbm,
    recent_hbm,
    readout_hbm,
    inmap_hbm,
    value_hbm,
    gate_hbm,
    step_hbm,
    project_hbm,
    states_hbm,
    tokens_out,
    fresh_out,
    recent_out,
    tokens_ref,
    norm_ref,
    bias_ref,
    rate_ref,
    skip_ref,
    gain_ref,
    taps_ref,
    recent_ref,
    w_in,
    w_step,
    w_out,
    state,
    spread,
    gather,
    part_send,
    part_recv,
    extra_send,
    extra_recv,
    gated_all,
    mixed_all,
    square_all,
    conv_ref,
    params_ref,
    chosen_ref,
    dec_ref,
    bm_ref,
    cm_ref,
    wide_ref,
    x_ref,
    small_sem,
    in_sem,
    step_sem,
    out_sem,
    state_sem,
    send_sem,
    extra_sem,
    part_sem,
    gated_sem,
    mixed_sem,
    square_sem,
):
    layers, groups, dp, tp, own, cols, heads, head_dim, span, features, width = dims
    me = lax.axis_index("dp")
    col = lax.axis_index("tp")
    members = dp // groups
    rows = members * own
    mine = groups - 1 - lax.rem(me, groups)
    place = me // groups

    def moved(k):
        if members & (members - 1):
            return lax.rem(place + k, members)
        return sum(
            lax.rem(place // bit + k // bit, 2) * bit
            for bit in (1 << power for power in range(members.bit_length() - 1)))

    def member(g, k):
        return moved(k) * groups + groups - 1 - g

    def slot(g, k):
        return k * groups + lax.rem(g - mine + groups, groups) - 1

    def column(k):
        return lax.rem(col + k + 1, tp)

    def columns(body):
        def at(index):
            pl.when(col + tp - index < tp)(lambda: body(col + tp - index))
            pl.when(col + index >= tp)(lambda: body(col + index - tp))

        each(tp, at, 1)

    small = [
        pltpu.make_async_copy(far, near, small_sem.at[index])
        for index, (far, near) in enumerate((
            (tokens_hbm, tokens_ref),
            (norm_hbm, norm_ref),
            (bias_hbm, bias_ref),
            (rate_hbm, rate_ref),
            (skip_hbm, skip_ref),
            (gain_hbm, gain_ref),
            (taps_hbm, taps_ref),
            (recent_hbm, recent_ref),
        ))
    ]
    sources = (readout_hbm, inmap_hbm, value_hbm, gate_hbm)
    filled = step_hbm.shape[1]

    def load_step(level):
        return pltpu.make_async_copy(
            step_hbm.at[level], w_step.at[level, :filled], step_sem.at[level])

    def load_in(level, w):
        return pltpu.make_async_copy(
            sources[w].at[level], w_in.at[level, w], in_sem.at[level, w])

    def load_out(level):
        return pltpu.make_async_copy(project_hbm.at[level], w_out.at[level], out_sem.at[level])

    def load_state(level):
        return pltpu.make_async_copy(states_hbm.at[level], state.at[level], state_sem.at[level])

    for copy in small[:2]:
        copy.start()
    load_step(0).start()
    load_in(0, 0).start()
    load_in(0, 1).start()

    barrier = pltpu.get_barrier_semaphore()
    each(dp, lambda k: pl.semaphore_signal(
        barrier, inc=1, device_id={"dp": lax.rem(me + k, dp)}, device_id_type=MESH), 1)
    each(tp - 1, lambda k: pl.semaphore_signal(
        barrier, inc=1, device_id={"tp": column(k)}, device_id_type=MESH))

    def send_extra(level, g, k):
        return pltpu.make_async_remote_copy(
            src_ref=extra_send.at[level, g, moved(k)],
            dst_ref=extra_recv.at[level, slot(g, k)],
            send_sem=send_sem.at[0],
            recv_sem=extra_sem.at[level],
            device_id={"dp": member(g, k)},
            device_id_type=MESH,
        )

    def send_part(level, w, g, k):
        return pltpu.make_async_remote_copy(
            src_ref=part_send.at[level, w, g, moved(k)],
            dst_ref=part_recv.at[level, w, slot(g, k)],
            send_sem=send_sem.at[1],
            recv_sem=part_sem.at[level, w],
            device_id={"dp": member(g, k)},
            device_id_type=MESH,
        )

    def send_gated(level, g, k):
        return pltpu.make_async_remote_copy(
            src_ref=gated_all.at[level, mine, place],
            dst_ref=gated_all.at[level, mine, place],
            send_sem=send_sem.at[2],
            recv_sem=gated_sem.at[level, mine],
            device_id={"dp": member(g, k)},
            device_id_type=MESH,
        )

    def send_mixed(level, g, target, origin):
        return pltpu.make_async_remote_copy(
            src_ref=mixed_all.at[level, g, origin],
            dst_ref=mixed_all.at[level, g, origin],
            send_sem=send_sem.at[3],
            recv_sem=mixed_sem.at[level, g],
            device_id={"tp": target},
            device_id_type=MESH,
        )

    def send_square(level, g, target, origin):
        return pltpu.make_async_remote_copy(
            src_ref=square_all.at[level, g, origin],
            dst_ref=square_all.at[level, g, origin],
            send_sem=send_sem.at[4],
            recv_sem=square_sem.at[level, g],
            device_id={"tp": target},
            device_id_type=MESH,
        )

    def arrived(ref, sem):
        pltpu.make_async_remote_copy(
            src_ref=ref,
            dst_ref=ref,
            send_sem=send_sem.at[0],
            recv_sem=sem,
            device_id={"dp": lax.rem(me + 1, dp)},
            device_id_type=MESH,
        ).wait_recv()

    def sent(ref, index):
        pltpu.make_async_remote_copy(
            src_ref=ref,
            dst_ref=ref,
            send_sem=send_sem.at[index],
            recv_sem=extra_sem.at[0],
            device_id={"dp": lax.rem(me + 1, dp)},
            device_id_type=MESH,
        ).wait_send()

    def others(which, body):
        def far(index):
            for g in which:
                body(g, members - index)

        each(members, far, 1)
        for g in which:
            if groups > 1:
                pl.when(mine != g)(functools.partial(body, g, 0))

    def every(level, w, which):
        others(which, lambda g, k: send_part(level, w, g, k).start())

    low = lax.broadcasted_iota(jnp.int32, (own, LANES), 1) < head_dim

    def twice(pair, odd):
        turned = pltpu.roll(pair, head_dim, 1)
        return jnp.where(low, turned, pair) if odd else jnp.where(low, pair, turned)

    def project_in(level, first, count):
        x = x_ref[first : first + count].reshape(count * rows, width)
        square = jnp.sum(x * x, axis=1, keepdims=True)
        gained = (x * norm_ref[level][None, :]).astype(BF16)
        lane = lax.broadcasted_iota(jnp.int32, (count * rows, LANES), 1)

        def store(w):
            part = jnp.dot(gained, w_in[level, w], preferred_element_type=F32)
            part_send[level, w, first : first + count] = part.reshape(
                count, members, own, cols).astype(BF16)

        if level == 0:
            with jax.named_scope(f"w_step_{level}"):
                load_step(level).wait()
        extra = lax.dot_general(
            gained, w_step[level], (((1,), (1,)), ((), ())), preferred_element_type=F32)
        extra = jnp.where(lane == LANES - 1, square, extra).reshape(count, members, own, LANES)
        high, rest = halves(extra)
        if level == 0:
            with jax.named_scope(f"w_in0_{level}"):
                load_in(level, 0).wait()
        extra_send[level, first : first + count, :, :, :LANES] = high
        extra_send[level, first : first + count, :, :, LANES:] = rest
        store(0)
        if level == 0 and first == 0:
            with jax.named_scope("barrier"):
                pl.semaphore_wait(barrier, dp - 1 + tp - 1)
        which = range(first, first + count)
        others(which, lambda g, k: send_extra(level, g, k).start())
        every(level, 0, which[:1])
        for w in range(1, 4):
            if level == 0:
                with jax.named_scope(f"w_in{w}_{level}"):
                    load_in(level, w).wait()
            store(w)
            with jax.named_scope(f"send{w}_{level}_{first}"):
                every(level, w, which[:1])
        for w in range(4):
            if count > 1:
                every(level, w, which[1:])

    def prepare():
        w_step[:, filled:] = jnp.zeros((layers, LANES - filled, width), BF16)

    def build():
        step = 256
        which = lax.broadcasted_iota(jnp.int32, (LANES, step), 0)
        entry = lax.broadcasted_iota(jnp.int32, (LANES, step), 1)
        across_lanes = lax.rem(which, head_dim) - entry // span
        which = lax.broadcasted_iota(jnp.int32, gather.shape, 1)
        entry = lax.broadcasted_iota(jnp.int32, gather.shape, 0)
        gather[...] = jnp.where(
            lax.rem(which, gather.shape[0] // span) == entry // span, 1.0, 0.0).astype(BF16)

        def fill(index, carry):
            start = pl.multiple_of(index * step, step)
            target = index * (step // span)
            spread[:, pl.ds(start, step)] = jnp.where(
                across_lanes == target, 1.0, 0.0).astype(BF16)
            return carry

        lax.fori_loop(0, head_dim * span // step, fill, 0)
        pick = lax.broadcasted_iota(jnp.int32, (LANES, cols), 0)
        slot = lax.broadcasted_iota(jnp.int32, (LANES, cols), 1)
        chosen_ref[...] = jnp.where(
            pick == col * heads + slot // head_dim, 1.0, 0.0).astype(BF16)
        pick = lax.broadcasted_iota(jnp.int32, (heads, cols), 0)
        slot = lax.broadcasted_iota(jnp.int32, (heads, cols), 1)
        wider = jnp.where(pick == slot // head_dim, 1.0, 0.0)
        for where, value in enumerate((bias_ref[...], jnp.exp(rate_ref[...]), skip_ref[...])):
            params_ref[where] = jnp.dot(
                value, wider, preferred_element_type=F32, precision=lax.Precision.HIGHEST)

    def convolve(level):
        for j in range(3):
            conv_ref[level, j] = jnp.sum(
                recent_ref[level, :, j].astype(F32)
                * taps_ref[: taps_ref.shape[0] - 1, j, level, :].astype(F32)[None],
                axis=1,
            )

    piece = 1024
    pieces = head_dim * span // piece

    def across(ref, h):
        return jnp.concatenate([ref[h]] * (piece // LANES), axis=1)

    def mix(level):
        with jax.named_scope(f"wr_extra_{level}"):
            arrived(extra_recv.at[level], extra_sem.at[level])
        load_state(level).wait()
        with jax.named_scope(f"wr_part0_{level}"):
            arrived(part_recv.at[level, READOUT], part_sem.at[level, READOUT])
        both = fold(
            dp - 1,
            lambda k, sum_in: sum_in + extra_recv[level, k].astype(F32),
            extra_send[level, mine, place].astype(F32),
        )
        total = both[:, :LANES] + both[:, LANES:]
        scale = lax.rsqrt(total[:, LANES - 1 :] / features + EPS)
        def await_part(w):
            with jax.named_scope(f"wr_part{w}_{level}"):
                arrived(part_recv.at[level, w], part_sem.at[level, w])

        def total_part(w):
            return scale * fold(
                dp - 1,
                lambda k, sum_in: sum_in + part_recv[level, w, k].astype(F32),
                part_send[level, w, mine, place].astype(F32),
            )

        fresh_u = {}

        def active(w, j):
            u = total_part(w).astype(BF16).astype(F32)
            fresh_u[j] = u
            return silu(
                conv_ref[level, j]
                + u * taps_ref[taps_ref.shape[0] - 1, j, level : level + 1, :].astype(F32))

        cm = active(READOUT, 2)
        for h in range(heads):
            window = slice(h // 2 * LANES, h // 2 * LANES + LANES)
            cm_ref[h] = twice(cm[:, window], h % 2)
        doubled = 2 * LANES
        chunks = head_dim * span // doubled
        read = jnp.concatenate([
            state[level, h, :, c * doubled : (c + 1) * doubled]
            * jnp.concatenate([cm_ref[h]] * 2, axis=1)
            for c in range(chunks) for h in range(heads)], axis=0).astype(BF16)
        read = jnp.dot(read, gather[...], preferred_element_type=F32)
        turn = lax.rem(
            lax.broadcasted_iota(jnp.int32, (heads * own, LANES), 1), head_dim) // (doubled // span)
        y = read[: heads * own]
        for c in range(1, chunks):
            y = jnp.where(turn == c, read[c * heads * own : (c + 1) * heads * own], y)
        chosen = chosen_ref[...]
        high, rest = halves(total * scale)
        raw = jnp.dot(high, chosen, preferred_element_type=F32) + jnp.dot(
            rest, chosen, preferred_element_type=F32)
        raw = raw + params_ref[0, level : level + 1, :]
        size = jnp.maximum(raw, 0.0) + jnp.log1p(jnp.exp(-jnp.abs(raw)))
        decay = jnp.exp(-size * params_ref[1, level : level + 1, :])

        await_part(INMAP)
        await_part(VALUE)
        bm = active(INMAP, 1)
        for h in range(heads):
            window = slice(h // 2 * LANES, h // 2 * LANES + LANES)
            dec_ref[h] = twice(decay[:, window], h % 2)
            bm_ref[h] = twice(bm[:, window], h % 2)
        xv = active(VALUE, 0)
        weighted = size * xv
        inner = []
        for h in range(heads):
            window = slice(h // 2 * LANES, h // 2 * LANES + LANES)
            one = twice(weighted[:, window], h % 2)
            high = one.astype(BF16).astype(F32)
            wide_ref[h * own : (h + 1) * own, :] = jnp.where(low, high, one - high)
            within = jnp.sum(
                jnp.where(low, bm_ref[h] * cm_ref[h], 0.0), axis=1, keepdims=True)
            inner.append(dec_ref[h] * y[h * own : (h + 1) * own] + one * within)
        y = jnp.concatenate(
            [jnp.where(low, inner[h], inner[h + 1]) for h in range(0, heads, 2)], axis=1)
        y = (y + params_ref[2, level : level + 1, :] * xv) * gain_ref[level : level + 1, :]
        await_part(GATE)
        gate = total_part(GATE)
        gated_all[level, mine, place] = (y * silu(gate)).astype(BF16)
        with jax.named_scope(f"s_gated_{level}"):
            others(range(groups), lambda g, k: send_gated(level, g, k).start())
        with jax.named_scope(f"advance_{level}"):
            wide = wide_ref[...].astype(BF16)

            def advance(index, carry):
                window = pl.ds(pl.multiple_of(index * piece, piece), piece)
                grown = jnp.dot(wide, spread[:, window], preferred_element_type=F32)
                for h in range(heads):
                    fresh_out[level, h, :, window] = (
                        across(dec_ref, h) * state[level, h, :, window]
                        + grown[h * own : (h + 1) * own] * across(bm_ref, h))
                return carry

            lax.fori_loop(0, pieces, advance, 0)
        with jax.named_scope(f"recent_{level}"):
            for j in range(3):
                kept = recent_ref[level, :, j].astype(F32)
                recent_out[level, :, j] = jnp.concatenate(
                    [kept[:, 1:], fresh_u[j][:, None]], axis=1).astype(BF16)

    cross = lax.broadcasted_iota(jnp.int32, (rows, rows), 0) == (
        lax.broadcasted_iota(jnp.int32, (rows, rows), 1))

    def project_out(level, g):
        if g == 0:
            load_out(level).wait()
        with jax.named_scope(f"wr_gated_{level}_{g}"):
            sem = gated_sem.at[level, g]
            if groups > 1:
                pl.when(mine == g)(lambda: arrived(gated_all.at[level, g, : members - 1], sem))
                pl.when(mine != g)(lambda: arrived(gated_all.at[level, g], sem))
            else:
                arrived(gated_all.at[level, g, : members - 1], sem)
        gated = gated_all[level, g].astype(F32).reshape(rows, cols)
        square = jnp.sum(gated * gated, axis=1, keepdims=True)
        square_all[level, g, col, :, :rows] = jnp.sum(
            jnp.where(cross, square, 0.0), axis=0, keepdims=True)
        mixed = jnp.dot(gated.astype(BF16), w_out[level], preferred_element_type=F32)
        mixed_all[level, g, col] = mixed.astype(BF16)
        columns(lambda target: send_square(level, g, target, col).start())
        with jax.named_scope(f"s_mixed_{level}_{g}"):
            columns(lambda target: send_mixed(level, g, target, col).start())

    def renew(level, g):
        arrived(square_all.at[level, g, : tp - 1], square_sem.at[level, g])
        square = fold(
            tp,
            lambda k, sum_in: sum_in + square_all[level, g, k, :, :rows],
            jnp.zeros((1, rows), F32),
        )
        scale = lax.rsqrt(square / (cols * tp) + EPS)
        scale = jnp.sum(jnp.where(cross, scale, 0.0), axis=1, keepdims=True)
        with jax.named_scope(f"wr_mixed_{level}_{g}"):
            arrived(mixed_all.at[level, g, : tp - 1], mixed_sem.at[level, g])
        mixed = fold(
            tp,
            lambda k, sum_in: sum_in + mixed_all[level, g, k].astype(F32),
            jnp.zeros((rows, width), F32),
        )
        fresh_x = (x_ref[g] + scale * mixed).astype(BF16)
        if level == layers - 1:
            for k in range(members):
                target = (k * groups + groups - 1 - g) * own
                tokens_out[target : target + own] = fresh_x[k * own : (k + 1) * own]
        else:
            x_ref[g] = fresh_x.astype(F32)

    prepare()
    with jax.named_scope("tokens"):
        small[0].wait()
        small[1].wait()
    load_in(0, 2).start()
    load_in(0, 3).start()
    for copy in small[2:]:
        copy.start()
    x = tokens_ref[...].astype(F32).reshape(members, groups, own, width)
    for g in range(groups):
        x_ref[g] = x[:, groups - 1 - g].reshape(rows, width)
    project_in(0, 0, groups)
    load_state(0).start()
    load_out(0).start()
    for level in range(1, layers):
        load_step(level).start()
        for w in range(4):
            load_in(level, w).start()
        load_state(level).start()
        load_out(level).start()
    with jax.named_scope("small_wait"):
        for copy in small[2:]:
            copy.wait()
    with jax.named_scope("build"):
        build()
        for level in range(layers):
            convolve(level)
    for level in range(layers):
        mix(level)
        for g in range(groups):
            project_out(level, g)
        if level < layers - 1:
            load_step(level + 1).wait()
            for w in range(4):
                load_in(level + 1, w).wait()
        for g in range(groups):
            renew(level, g)
            if level < layers - 1:
                project_in(level + 1, g, 1)

    sent(extra_recv, 0)
    sent(part_recv, 1)
    sent(part_recv.at[:, 0], 2)
    sent(mixed_all.at[:, :, : tp - 1], 3)
    sent(square_all.at[:, :, : tp - 1], 4)


def finish(tokens_ref, fresh_ref, recent_ref, tokens_hbm, fresh_hbm, recent_hbm, sem):
    layers, heads = fresh_ref.shape[:2]
    for level in range(layers):
        for h in range(heads):
            pltpu.make_async_copy(
                fresh_ref.at[level, h], fresh_hbm.at[level, h], sem.at[0]).start()
    small = (
        pltpu.make_async_copy(tokens_ref, tokens_hbm, sem.at[1]),
        pltpu.make_async_copy(recent_ref, recent_hbm, sem.at[2]),
    )
    for copy in small:
        copy.start()
    for copy in small:
        copy.wait()
    pltpu.make_async_copy(fresh_ref, fresh_hbm, sem.at[0]).wait()


def per_device(
    dp,
    tp,
    tokens,
    norm_gain,
    w_gate,
    w_value,
    w_inmap,
    w_readout,
    w_step,
    step_bias,
    decay_log,
    skip_gain,
    conv_taps,
    gate_gain,
    w_project,
    states,
    recent,
):
    layers, own, heads, entries = states.shape
    cols = w_gate.shape[2]
    head_dim = cols // heads
    span = entries // head_dim
    width = tokens.shape[1]
    features = width * dp
    groups = GROUPS if dp % GROUPS == 0 else 1
    dims = (layers, groups, dp, tp, own, cols, heads, head_dim, span, features, width)
    total = tokens.shape[0]
    rows = total // groups

    vmem = pl.BlockSpec(memory_space=pltpu.VMEM)
    anywhere = pl.BlockSpec(memory_space=pltpu.HBM)
    turned = recent.transpose(0, 1, 3, 2, 4)
    taps = conv_taps.transpose(1, 2, 0, 3)
    dma = pltpu.SemaphoreType.DMA
    padded = -(-rows // LANES) * LANES
    kept_bytes = 2 * tokens.size + 4 * states.size + 2 * recent.size
    results = pl.pallas_call(
        functools.partial(kernel, dims),
        out_shape=(
            pltpu.VMEM((total, width), BF16),
            pltpu.VMEM((layers, heads, own, entries), F32),
            pltpu.VMEM(turned.shape, BF16),
        ),
        in_specs=[anywhere] * 15,
        out_specs=(vmem, vmem, vmem),
        scratch_shapes=[
            pltpu.VMEM(tokens.shape, BF16),
            pltpu.VMEM(norm_gain.shape, F32),
            pltpu.VMEM(step_bias.shape, F32),
            pltpu.VMEM(decay_log.shape, F32),
            pltpu.VMEM(skip_gain.shape, F32),
            pltpu.VMEM(gate_gain.shape, F32),
            pltpu.VMEM(taps.shape, BF16),
            pltpu.VMEM(turned.shape, BF16),
            pltpu.VMEM((layers, 4, width, cols), BF16),
            pltpu.VMEM((layers, LANES, width), BF16),
            pltpu.VMEM((layers, cols, width), BF16),
            pltpu.VMEM((layers, heads, own, entries), F32),
            pltpu.VMEM((LANES, entries), BF16),
            pltpu.VMEM((2 * LANES, LANES), BF16),
            pltpu.VMEM((layers, 4, groups, dp // groups, own, cols), BF16),
            pltpu.VMEM((layers, 4, dp - 1, own, cols), BF16),
            pltpu.VMEM((layers, groups, dp // groups, own, 2 * LANES), BF16),
            pltpu.VMEM((layers, dp - 1, own, 2 * LANES), BF16),
            pltpu.VMEM((layers, groups, dp // groups, own, cols), BF16),
            pltpu.VMEM((layers, groups, tp, rows, width), BF16),
            pltpu.VMEM((layers, groups, tp, 1, padded), F32),
            pltpu.VMEM((layers, 3, own, cols), F32),
            pltpu.VMEM((3, layers, cols), F32),
            pltpu.VMEM((LANES, cols), BF16),
            pltpu.VMEM((heads, own, LANES), F32),
            pltpu.VMEM((heads, own, LANES), F32),
            pltpu.VMEM((heads, own, LANES), F32),
            pltpu.VMEM((heads * own, LANES), F32),
            pltpu.VMEM((groups, rows, width), F32),
            dma((8,)),
            dma((layers, 4)),
            dma((layers,)),
            dma((layers,)),
            dma((layers,)),
            dma((5,)),
            dma((layers,)),
            dma((layers, 4)),
            dma((layers, groups)),
            dma((layers, groups)),
            dma((layers, groups)),
        ],
        compiler_params=pltpu.CompilerParams(
            collective_id=0, has_side_effects=True, vmem_limit_bytes=VMEM_BYTES - kept_bytes),
    )(
        tokens,
        norm_gain,
        step_bias,
        decay_log,
        skip_gain,
        gate_gain,
        taps,
        turned,
        w_readout,
        w_inmap,
        w_value,
        w_gate,
        w_step.transpose(0, 2, 1),
        w_project,
        states.transpose(0, 2, 1, 3),
    )
    out_tokens, fresh, kept = pl.pallas_call(
        finish,
        out_shape=(
            jax.ShapeDtypeStruct((total, width), BF16),
            jax.ShapeDtypeStruct((layers, heads, own, entries), F32),
            jax.ShapeDtypeStruct(turned.shape, BF16),
        ),
        in_specs=[vmem] * 3,
        out_specs=(anywhere,) * 3,
        scratch_shapes=[dma((3,))],
        compiler_params=pltpu.CompilerParams(vmem_limit_bytes=16 * 1024 * 1024),
    )(*results)
    next_states = fresh.transpose(0, 2, 1, 3)
    next_recent = kept.transpose(0, 1, 3, 2, 4)
    return out_tokens, next_states, next_recent


GROUPS = 2
def solution(mesh):
    in_specs = (
        P(None, "dp"),
        P(None, "dp"),
        P(None, "dp", "tp"),
        P(None, "dp", "tp"),
        P(None, "dp", "tp"),
        P(None, "dp", "tp"),
        P(None, "dp", None),
        P(None, "tp"),
        P(None, "tp"),
        P(None, "tp"),
        P(None, None, None, "tp"),
        P(None, "tp"),
        P(None, "tp", "dp"),
        P(None, "dp", "tp", None),
        P(None, "dp", None, None, "tp"),
    )
    out_specs = (P(None, "dp"), P(None, "dp", "tp", None), P(None, "dp", None, None, "tp"))
    body = functools.partial(per_device, mesh.shape["dp"], mesh.shape["tp"])
    return jax.shard_map(
        body, mesh=mesh, in_specs=in_specs, out_specs=out_specs, check_vma=False
    )
```

```python
import functools

import jax
import jax.numpy as jnp
from jax import lax
from jax.experimental import pallas as pl
from jax.experimental.pallas import tpu as pltpu
from jax.sharding import PartitionSpec as P

EPS = 1e-06
LANES = 128
MESH = pl.DeviceIdType.MESH
F32 = jnp.float32
BF16 = jnp.bfloat16
VMEM_BYTES = 67043328
READOUT, INMAP, VALUE, GATE = range(4)


def each(count, body, first=0):
    if count - first <= 8:
        for index in range(first, count):
            body(index)
    else:
        lax.fori_loop(first, count, lambda index, carry: (body(index), carry)[1], 0)


def fold(count, body, start, first=0):
    if count - first <= 8:
        for index in range(first, count):
            start = body(index, start)
        return start
    return lax.fori_loop(first, count, body, start)


def silu(value):
    return value / (1.0 + jnp.exp(-value))


def halves(value):
    high = value.astype(BF16)
    return high, (value - high.astype(F32)).astype(BF16)


def kernel(
    dims,
    tokens_hbm,
    norm_hbm,
    bias_hbm,
    rate_hbm,
    skip_hbm,
    gain_hbm,
    taps_hbm,
    recent_hbm,
    readout_hbm,
    inmap_hbm,
    value_hbm,
    gate_hbm,
    step_hbm,
    project_hbm,
    states_hbm,
    tokens_out,
    fresh_out,
    recent_out,
    tokens_ref,
    norm_ref,
    head_ref,
    gain_ref,
    taps_ref,
    recent_ref,
    w_in,
    w_step,
    w_out,
    state,
    spread,
    gather,
    part_send,
    part_recv,
    first_send,
    first_recv,
    gated_all,
    mixed_all,
    square_all,
    conv_ref,
    params_ref,
    chosen_ref,
    dec_ref,
    bm_ref,
    cm_ref,
    wide_ref,
    x_ref,
    small_sem,
    in_sem,
    bulk_sem,
    send_sem,
    first_sem,
    part_sem,
    gated_sem,
    mixed_sem,
    square_sem,
):
    layers, groups, dp, tp, own, cols, heads, head_dim, span, features, width = dims
    me = lax.axis_index("dp")
    col = lax.axis_index("tp")
    members = dp // groups
    rows = members * own
    mine = groups - 1 - lax.rem(me, groups)
    place = me // groups

    def moved(k):
        if members & (members - 1):
            return lax.rem(place + k, members)
        return sum(
            lax.rem(place // bit + k // bit, 2) * bit
            for bit in (1 << power for power in range(members.bit_length() - 1)))

    def member(g, k):
        return moved(k) * groups + groups - 1 - g

    def slot(g, k):
        return k * groups + lax.rem(g - mine + groups, groups) - 1

    def column(k):
        return lax.rem(col + k + 1, tp)

    def columns(body):
        def at(index):
            pl.when(col + tp - index < tp)(lambda: body(col + tp - index))
            pl.when(col + index >= tp)(lambda: body(col + index - tp))

        each(tp, at, 1)

    small = [
        pltpu.make_async_copy(far, near, small_sem.at[index])
        for index, (far, near) in enumerate((
            (tokens_hbm, tokens_ref),
            (norm_hbm, norm_ref),
            (gain_hbm, gain_ref),
            (taps_hbm, taps_ref),
            (recent_hbm, recent_ref),
        ))
    ]
    heads_sem = small_sem.at[len(small)]
    per_head = [
        pltpu.make_async_copy(far, head_ref.at[index], heads_sem)
        for index, far in enumerate((bias_hbm, rate_hbm, skip_hbm))
    ]
    sources = (readout_hbm, inmap_hbm, value_hbm, gate_hbm)
    filled = step_hbm.shape[1]

    load_step = pltpu.make_async_copy(step_hbm, w_step.at[:, :filled], bulk_sem.at[0])
    load_out = pltpu.make_async_copy(project_hbm, w_out, bulk_sem.at[1])
    load_state = pltpu.make_async_copy(states_hbm, state, bulk_sem.at[2])

    def load_in(level, w):
        return pltpu.make_async_copy(
            sources[w].at[level], w_in.at[level, w], in_sem.at[w if level == 0 else level + 3])

    def await_in(level):
        pltpu.make_async_copy(w_in.at[level], w_in.at[level], in_sem.at[level + 3]).wait()

    for copy in small[:2]:
        copy.start()
    load_step.start()
    load_in(0, 0).start()
    load_in(0, 1).start()

    barrier = pltpu.get_barrier_semaphore()
    each(dp, lambda k: pl.semaphore_signal(
        barrier, inc=1, device_id={"dp": lax.rem(me + k, dp)}, device_id_type=MESH), 1)
    each(tp - 1, lambda k: pl.semaphore_signal(
        barrier, inc=1, device_id={"tp": column(k)}, device_id_type=MESH))

    def send_first(level, g, k):
        return pltpu.make_async_remote_copy(
            src_ref=first_send.at[level, g, moved(k)],
            dst_ref=first_recv.at[level, slot(g, k)],
            send_sem=send_sem.at[0],
            recv_sem=first_sem.at[level],
            device_id={"dp": member(g, k)},
            device_id_type=MESH,
        )

    def send_part(level, w, g, k):
        return pltpu.make_async_remote_copy(
            src_ref=part_send.at[level, w - 1, g, moved(k)],
            dst_ref=part_recv.at[level, w - 1, slot(g, k)],
            send_sem=send_sem.at[1],
            recv_sem=part_sem.at[level, w // GATE],
            device_id={"dp": member(g, k)},
            device_id_type=MESH,
        )

    def send_gated(level, g, k):
        return pltpu.make_async_remote_copy(
            src_ref=gated_all.at[level, mine, place],
            dst_ref=gated_all.at[level, mine, place],
            send_sem=send_sem.at[2],
            recv_sem=gated_sem.at[level, mine],
            device_id={"dp": member(g, k)},
            device_id_type=MESH,
        )

    def send_mixed(level, g, target, origin):
        return pltpu.make_async_remote_copy(
            src_ref=mixed_all.at[level, g, origin],
            dst_ref=mixed_all.at[level, g, origin],
            send_sem=send_sem.at[3],
            recv_sem=mixed_sem.at[level, g],
            device_id={"tp": target},
            device_id_type=MESH,
        )

    def send_square(level, g, target, origin):
        return pltpu.make_async_remote_copy(
            src_ref=square_all.at[level, g, origin],
            dst_ref=square_all.at[level, g, origin],
            send_sem=send_sem.at[4],
            recv_sem=square_sem.at[level, g],
            device_id={"tp": target},
            device_id_type=MESH,
        )

    def arrived(ref, sem):
        pltpu.make_async_remote_copy(
            src_ref=ref,
            dst_ref=ref,
            send_sem=send_sem.at[0],
            recv_sem=sem,
            device_id={"dp": lax.rem(me + 1, dp)},
            device_id_type=MESH,
        ).wait_recv()

    def sent(ref, index):
        pltpu.make_async_remote_copy(
            src_ref=ref,
            dst_ref=ref,
            send_sem=send_sem.at[index],
            recv_sem=first_sem.at[0],
            device_id={"dp": lax.rem(me + 1, dp)},
            device_id_type=MESH,
        ).wait_send()

    def others(which, body):
        def far(index):
            for g in which:
                body(g, members - index)

        each(members, far, 1)
        for g in which:
            if groups > 1:
                pl.when(mine != g)(functools.partial(body, g, 0))

    def every(level, w, which):
        others(which, lambda g, k: send_part(level, w, g, k).start())

    low = lax.broadcasted_iota(jnp.int32, (own, LANES), 1) < head_dim

    def twice(pair, odd):
        turned = pltpu.roll(pair, head_dim, 1)
        return jnp.where(low, turned, pair) if odd else jnp.where(low, pair, turned)

    def project_in(level, first, count):
        x = x_ref[first : first + count].reshape(count * rows, width)
        square = jnp.sum(x * x, axis=1, keepdims=True)
        gained = (x * norm_ref[level][None, :]).astype(BF16)
        lane = lax.broadcasted_iota(jnp.int32, (count * rows, LANES), 1)

        def store(w):
            part = jnp.dot(gained, w_in[level, w], preferred_element_type=F32)
            part = part.reshape(count, members, own, cols).astype(BF16)
            if w == READOUT:
                first_send[level, first : first + count, :, :, :cols] = part
            else:
                part_send[level, w - 1, first : first + count] = part

        if level == 0:
            with jax.named_scope(f"w_step_{level}"):
                load_step.wait()
        extra = lax.dot_general(
            gained, w_step[level], (((1,), (1,)), ((), ())), preferred_element_type=F32)
        extra = jnp.where(lane == LANES - 1, square, extra).reshape(count, members, own, LANES)
        high, rest = halves(extra)
        if level == 0:
            with jax.named_scope(f"w_in0_{level}"):
                load_in(level, 0).wait()
        first_send[level, first : first + count, :, :, cols : cols + LANES] = high
        first_send[level, first : first + count, :, :, cols + LANES :] = rest
        store(0)
        if level == 0 and first == 0:
            with jax.named_scope("barrier"):
                pl.semaphore_wait(barrier, dp - 1 + tp - 1)
        which = range(first, first + count)
        others(which[:1], lambda g, k: send_first(level, g, k).start())
        for w in range(1, 4):
            if level == 0:
                with jax.named_scope(f"w_in{w}_{level}"):
                    load_in(level, w).wait()
            store(w)
            with jax.named_scope(f"send{w}_{level}_{first}"):
                every(level, w, which[:1])

    def prepare():
        w_step[:, filled:] = jnp.zeros((layers, LANES - filled, width), BF16)

    def build():
        step = 256
        which = lax.broadcasted_iota(jnp.int32, (LANES, step), 0)
        entry = lax.broadcasted_iota(jnp.int32, (LANES, step), 1)
        across_lanes = lax.rem(which, head_dim) - entry // span
        which = lax.broadcasted_iota(jnp.int32, gather.shape, 1)
        entry = lax.broadcasted_iota(jnp.int32, gather.shape, 0)
        gather[...] = jnp.where(
            lax.rem(which, gather.shape[0] // span) == entry // span, 1.0, 0.0).astype(BF16)

        def fill(index, carry):
            start = pl.multiple_of(index * step, step)
            target = index * (step // span)
            spread[:, pl.ds(start, step)] = jnp.where(
                across_lanes == target, 1.0, 0.0).astype(BF16)
            return carry

        lax.fori_loop(0, head_dim * span // step, fill, 0)
        pick = lax.broadcasted_iota(jnp.int32, (LANES, cols), 0)
        slot = lax.broadcasted_iota(jnp.int32, (LANES, cols), 1)
        chosen_ref[...] = jnp.where(
            pick == col * heads + slot // head_dim, 1.0, 0.0).astype(BF16)
        pick = lax.broadcasted_iota(jnp.int32, (heads, cols), 0)
        slot = lax.broadcasted_iota(jnp.int32, (heads, cols), 1)
        wider = jnp.where(pick == slot // head_dim, 1.0, 0.0)
        for where, value in enumerate((head_ref[0], jnp.exp(head_ref[1]), head_ref[2])):
            params_ref[where] = jnp.dot(
                value, wider, preferred_element_type=F32, precision=lax.Precision.HIGHEST)

    def convolve(level):
        for j in range(3):
            conv_ref[level, j] = jnp.sum(
                recent_ref[level, :, j].astype(F32)
                * taps_ref[: taps_ref.shape[0] - 1, j, level, :].astype(F32)[None],
                axis=1,
            )

    piece = 1024
    pieces = head_dim * span // piece

    def across(ref, h):
        return jnp.concatenate([ref[h]] * (piece // LANES), axis=1)

    def mix(level):
        with jax.named_scope(f"wr_extra_{level}"):
            arrived(first_recv.at[level], first_sem.at[level])
        if level == 0:
            load_state.wait()
        both = fold(
            dp - 1,
            lambda k, sum_in: sum_in + first_recv[level, k].astype(F32),
            first_send[level, mine, place].astype(F32),
        )
        readout = both[:, :cols]
        total = both[:, cols : cols + LANES] + both[:, cols + LANES :]
        scale = lax.rsqrt(total[:, LANES - 1 :] / features + EPS)
        def total_part(w):
            return fold(
                dp - 1,
                lambda k, sum_in: sum_in + part_recv[level, w - 1, k].astype(F32),
                part_send[level, w - 1, mine, place].astype(F32),
            )

        fresh_u = {}

        def active(summed, j):
            u = (scale * summed).astype(BF16).astype(F32)
            fresh_u[j] = u
            return silu(
                conv_ref[level, j]
                + u * taps_ref[taps_ref.shape[0] - 1, j, level : level + 1, :].astype(F32))

        cm = active(readout, 2)
        for h in range(heads):
            window = slice(h // 2 * LANES, h // 2 * LANES + LANES)
            cm_ref[h] = twice(cm[:, window], h % 2)
        doubled = 2 * LANES
        chunks = head_dim * span // doubled
        read = jnp.concatenate([
            state[level, h, :, c * doubled : (c + 1) * doubled]
            * jnp.concatenate([cm_ref[h]] * 2, axis=1)
            for c in range(chunks) for h in range(heads)], axis=0).astype(BF16)
        read = jnp.dot(read, gather[...], preferred_element_type=F32)
        turn = lax.rem(
            lax.broadcasted_iota(jnp.int32, (heads * own, LANES), 1), head_dim) // (doubled // span)
        y = read[: heads * own]
        for c in range(1, chunks):
            y = jnp.where(turn == c, read[c * heads * own : (c + 1) * heads * own], y)
        chosen = chosen_ref[...]
        high, rest = halves(total * scale)
        raw = jnp.dot(high, chosen, preferred_element_type=F32) + jnp.dot(
            rest, chosen, preferred_element_type=F32)
        raw = raw + params_ref[0, level : level + 1, :]
        size = jnp.maximum(raw, 0.0) + jnp.log1p(jnp.exp(-jnp.abs(raw)))
        decay = jnp.exp(-size * params_ref[1, level : level + 1, :])

        with jax.named_scope(f"wr_part_{level}"):
            arrived(part_recv.at[level, : GATE - 1], part_sem.at[level, 0])
        bm = active(total_part(INMAP), 1)
        for h in range(heads):
            window = slice(h // 2 * LANES, h // 2 * LANES + LANES)
            dec_ref[h] = twice(decay[:, window], h % 2)
            bm_ref[h] = twice(bm[:, window], h % 2)
        xv = active(total_part(VALUE), 0)
        weighted = size * xv
        inner = []
        for h in range(heads):
            window = slice(h // 2 * LANES, h // 2 * LANES + LANES)
            one = twice(weighted[:, window], h % 2)
            high = one.astype(BF16).astype(F32)
            wide_ref[h * own : (h + 1) * own, :] = jnp.where(low, high, one - high)
            within = jnp.sum(
                jnp.where(low, bm_ref[h] * cm_ref[h], 0.0), axis=1, keepdims=True)
            inner.append(dec_ref[h] * y[h * own : (h + 1) * own] + one * within)
        y = jnp.concatenate(
            [jnp.where(low, inner[h], inner[h + 1]) for h in range(0, heads, 2)], axis=1)
        y = (y + params_ref[2, level : level + 1, :] * xv) * gain_ref[level : level + 1, :]
        with jax.named_scope(f"wr_gate_{level}"):
            arrived(part_recv.at[level, GATE - 1], part_sem.at[level, 1])
        gate = scale * total_part(GATE)
        gated_all[level, mine, place] = (y * silu(gate)).astype(BF16)
        with jax.named_scope(f"s_gated_{level}"):
            others(range(groups), lambda g, k: send_gated(level, g, k).start())
        with jax.named_scope(f"advance_{level}"):
            wide = wide_ref[...].astype(BF16)

            def advance(index, carry):
                window = pl.ds(pl.multiple_of(index * piece, piece), piece)
                grown = jnp.dot(wide, spread[:, window], preferred_element_type=F32)
                for h in range(heads):
                    fresh_out[level, h, :, window] = (
                        across(dec_ref, h) * state[level, h, :, window]
                        + grown[h * own : (h + 1) * own] * across(bm_ref, h))
                return carry

            lax.fori_loop(0, pieces, advance, 0)
        with jax.named_scope(f"recent_{level}"):
            for j in range(3):
                kept = recent_ref[level, :, j].astype(F32)
                recent_out[level, :, j] = jnp.concatenate(
                    [kept[:, 1:], fresh_u[j][:, None]], axis=1).astype(BF16)

    cross = lax.broadcasted_iota(jnp.int32, (rows, rows), 0) == (
        lax.broadcasted_iota(jnp.int32, (rows, rows), 1))

    def project_out(level, g):
        if level == 0 and g == 0:
            load_out.wait()
        with jax.named_scope(f"wr_gated_{level}_{g}"):
            sem = gated_sem.at[level, g]
            if groups > 1:
                pl.when(mine == g)(lambda: arrived(gated_all.at[level, g, : members - 1], sem))
                pl.when(mine != g)(lambda: arrived(gated_all.at[level, g], sem))
            else:
                arrived(gated_all.at[level, g, : members - 1], sem)
        gated = gated_all[level, g].astype(F32).reshape(rows, cols)
        square = jnp.sum(gated * gated, axis=1, keepdims=True)
        square_all[level, g, col, :, :rows] = jnp.sum(
            jnp.where(cross, square, 0.0), axis=0, keepdims=True)
        mixed = jnp.dot(gated.astype(BF16), w_out[level], preferred_element_type=F32)
        mixed_all[level, g, col] = mixed.astype(BF16)
        columns(lambda target: send_square(level, g, target, col).start())
        with jax.named_scope(f"s_mixed_{level}_{g}"):
            columns(lambda target: send_mixed(level, g, target, col).start())

    def renew(level, g):
        arrived(square_all.at[level, g, : tp - 1], square_sem.at[level, g])
        square = fold(
            tp,
            lambda k, sum_in: sum_in + square_all[level, g, k, :, :rows],
            jnp.zeros((1, rows), F32),
        )
        scale = lax.rsqrt(square / (cols * tp) + EPS)
        scale = jnp.sum(jnp.where(cross, scale, 0.0), axis=1, keepdims=True)
        with jax.named_scope(f"wr_mixed_{level}_{g}"):
            arrived(mixed_all.at[level, g, : tp - 1], mixed_sem.at[level, g])
        mixed = fold(
            tp,
            lambda k, sum_in: sum_in + mixed_all[level, g, k].astype(F32),
            jnp.zeros((rows, width), F32),
        )
        fresh_x = (x_ref[g] + scale * mixed).astype(BF16)
        if level == layers - 1:
            for k in range(members):
                target = (k * groups + groups - 1 - g) * own
                tokens_out[target : target + own] = fresh_x[k * own : (k + 1) * own]
        else:
            x_ref[g] = fresh_x.astype(F32)

    prepare()
    with jax.named_scope("tokens"):
        small[0].wait()
        small[1].wait()
    load_in(0, 2).start()
    load_in(0, 3).start()
    for copy in small[2:] + per_head:
        copy.start()
    x = tokens_ref[...].astype(F32).reshape(members, groups, own, width)
    for g in range(groups):
        x_ref[g] = x[:, groups - 1 - g].reshape(rows, width)
    project_in(0, 0, groups)
    load_state.start()
    load_out.start()
    for level in range(1, layers):
        for w in range(4):
            load_in(level, w).start()
    def rest():
        if groups > 1:
            others(range(1, groups), lambda g, k: send_first(0, g, k).start())
            for w in range(1, 4):
                every(0, w, range(1, groups))

    with jax.named_scope("small_wait"):
        for copy in small[2:]:
            copy.wait()
        pltpu.make_async_copy(head_ref, head_ref, heads_sem).wait()
    with jax.named_scope("build"):
        build()
        for level in range(layers):
            convolve(level)
        rest()
    for level in range(layers):
        mix(level)
        for g in range(groups):
            project_out(level, g)
        if level < layers - 1:
            await_in(level + 1)
        for g in range(groups):
            renew(level, g)
            if level < layers - 1:
                project_in(level + 1, g, 1)

    sent(first_recv, 0)
    sent(part_recv, 1)
    sent(part_recv.at[:, 0], 2)
    sent(mixed_all.at[:, :, : tp - 1], 3)
    sent(square_all.at[:, :, : tp - 1], 4)


def finish(tokens_ref, fresh_ref, recent_ref, tokens_hbm, fresh_hbm, recent_hbm, sem):
    layers, heads = fresh_ref.shape[:2]
    for level in range(layers):
        for h in range(heads):
            pltpu.make_async_copy(
                fresh_ref.at[level, h], fresh_hbm.at[level, h], sem.at[0]).start()
    small = (
        pltpu.make_async_copy(tokens_ref, tokens_hbm, sem.at[1]),
        pltpu.make_async_copy(recent_ref, recent_hbm, sem.at[2]),
    )
    for copy in small:
        copy.start()
    for copy in small:
        copy.wait()
    pltpu.make_async_copy(fresh_ref, fresh_hbm, sem.at[0]).wait()


def per_device(
    dp,
    tp,
    tokens,
    norm_gain,
    w_gate,
    w_value,
    w_inmap,
    w_readout,
    w_step,
    step_bias,
    decay_log,
    skip_gain,
    conv_taps,
    gate_gain,
    w_project,
    states,
    recent,
):
    layers, own, heads, entries = states.shape
    cols = w_gate.shape[2]
    head_dim = cols // heads
    span = entries // head_dim
    width = tokens.shape[1]
    features = width * dp
    groups = GROUPS if dp % GROUPS == 0 else 1
    dims = (layers, groups, dp, tp, own, cols, heads, head_dim, span, features, width)
    total = tokens.shape[0]
    rows = total // groups

    vmem = pl.BlockSpec(memory_space=pltpu.VMEM)
    anywhere = pl.BlockSpec(memory_space=pltpu.HBM)
    turned = recent.transpose(0, 1, 3, 2, 4)
    taps = conv_taps.transpose(1, 2, 0, 3)
    dma = pltpu.SemaphoreType.DMA
    padded = -(-rows // LANES) * LANES
    kept_bytes = 2 * tokens.size + 4 * states.size + 2 * recent.size
    results = pl.pallas_call(
        functools.partial(kernel, dims),
        out_shape=(
            pltpu.VMEM((total, width), BF16),
            pltpu.VMEM((layers, heads, own, entries), F32),
            pltpu.VMEM(turned.shape, BF16),
        ),
        in_specs=[anywhere] * 15,
        out_specs=(vmem, vmem, vmem),
        scratch_shapes=[
            pltpu.VMEM(tokens.shape, BF16),
            pltpu.VMEM(norm_gain.shape, F32),
            pltpu.VMEM((3,) + step_bias.shape, F32),
            pltpu.VMEM(gate_gain.shape, F32),
            pltpu.VMEM(taps.shape, BF16),
            pltpu.VMEM(turned.shape, BF16),
            pltpu.VMEM((layers, 4, width, cols), BF16),
            pltpu.VMEM((layers, LANES, width), BF16),
            pltpu.VMEM((layers, cols, width), BF16),
            pltpu.VMEM((layers, heads, own, entries), F32),
            pltpu.VMEM((LANES, entries), BF16),
            pltpu.VMEM((2 * LANES, LANES), BF16),
            pltpu.VMEM((layers, 3, groups, dp // groups, own, cols), BF16),
            pltpu.VMEM((layers, 3, dp - 1, own, cols), BF16),
            pltpu.VMEM((layers, groups, dp // groups, own, cols + 2 * LANES), BF16),
            pltpu.VMEM((layers, dp - 1, own, cols + 2 * LANES), BF16),
            pltpu.VMEM((layers, groups, dp // groups, own, cols), BF16),
            pltpu.VMEM((layers, groups, tp, rows, width), BF16),
            pltpu.VMEM((layers, groups, tp, 1, padded), F32),
            pltpu.VMEM((layers, 3, own, cols), F32),
            pltpu.VMEM((3, layers, cols), F32),
            pltpu.VMEM((LANES, cols), BF16),
            pltpu.VMEM((heads, own, LANES), F32),
            pltpu.VMEM((heads, own, LANES), F32),
            pltpu.VMEM((heads, own, LANES), F32),
            pltpu.VMEM((heads * own, LANES), F32),
            pltpu.VMEM((groups, rows, width), F32),
            dma((6,)),
            dma((layers + 3,)),
            dma((3,)),
            dma((5,)),
            dma((layers,)),
            dma((layers, 2)),
            dma((layers, groups)),
            dma((layers, groups)),
            dma((layers, groups)),
        ],
        compiler_params=pltpu.CompilerParams(
            collective_id=0, has_side_effects=True, vmem_limit_bytes=VMEM_BYTES - kept_bytes),
    )(
        tokens,
        norm_gain,
        step_bias,
        decay_log,
        skip_gain,
        gate_gain,
        taps,
        turned,
        w_readout,
        w_inmap,
        w_value,
        w_gate,
        w_step.transpose(0, 2, 1),
        w_project,
        states.transpose(0, 2, 1, 3),
    )
    out_tokens, fresh, kept = pl.pallas_call(
        finish,
        out_shape=(
            jax.ShapeDtypeStruct((total, width), BF16),
            jax.ShapeDtypeStruct((layers, heads, own, entries), F32),
            jax.ShapeDtypeStruct(turned.shape, BF16),
        ),
        in_specs=[vmem] * 3,
        out_specs=(anywhere,) * 3,
        scratch_shapes=[dma((3,))],
        compiler_params=pltpu.CompilerParams(vmem_limit_bytes=16 * 1024 * 1024),
    )(*results)
    next_states = fresh.transpose(0, 2, 1, 3)
    next_recent = kept.transpose(0, 1, 3, 2, 4)
    return out_tokens, next_states, next_recent


GROUPS = 2
def solution(mesh):
    in_specs = (
        P(None, "dp"),
        P(None, "dp"),
        P(None, "dp", "tp"),
        P(None, "dp", "tp"),
        P(None, "dp", "tp"),
        P(None, "dp", "tp"),
        P(None, "dp", None),
        P(None, "tp"),
        P(None, "tp"),
        P(None, "tp"),
        P(None, None, None, "tp"),
        P(None, "tp"),
        P(None, "tp", "dp"),
        P(None, "dp", "tp", None),
        P(None, "dp", None, None, "tp"),
    )
    out_specs = (P(None, "dp"), P(None, "dp", "tp", None), P(None, "dp", None, None, "tp"))
    body = functools.partial(per_device, mesh.shape["dp"], mesh.shape["tp"])
    return jax.shard_map(
        body, mesh=mesh, in_specs=in_specs, out_specs=out_specs, check_vma=False
    )
```

```python
import functools

import jax
import jax.numpy as jnp
from jax import lax
from jax.experimental import pallas as pl
from jax.experimental.pallas import tpu as pltpu
from jax.sharding import PartitionSpec as P

EPS = 1e-06
LANES = 128
MESH = pl.DeviceIdType.MESH
F32 = jnp.float32
BF16 = jnp.bfloat16
VMEM_BYTES = 67043328
READOUT, INMAP, VALUE, GATE = range(4)


def each(count, body, first=0):
    if count - first <= 8:
        for index in range(first, count):
            body(index)
    else:
        lax.fori_loop(first, count, lambda index, carry: (body(index), carry)[1], 0)


def fold(count, body, start, first=0):
    if count - first <= 8:
        for index in range(first, count):
            start = body(index, start)
        return start
    return lax.fori_loop(first, count, body, start)


def silu(value):
    return value / (1.0 + jnp.exp(-value))


def halves(value):
    high = value.astype(BF16)
    return high, (value - high.astype(F32)).astype(BF16)


def kernel(
    dims,
    tokens_hbm,
    norm_hbm,
    bias_hbm,
    rate_hbm,
    skip_hbm,
    gain_hbm,
    taps_hbm,
    recent_hbm,
    readout_hbm,
    inmap_hbm,
    value_hbm,
    gate_hbm,
    step_hbm,
    project_hbm,
    states_hbm,
    tokens_out,
    fresh_out,
    recent_out,
    tokens_ref,
    norm_ref,
    head_ref,
    gain_ref,
    taps_ref,
    recent_ref,
    w_in,
    w_step,
    w_out,
    state,
    spread,
    gather,
    part_send,
    part_recv,
    first_send,
    first_recv,
    gated_all,
    mixed_all,
    square_all,
    conv_ref,
    params_ref,
    chosen_ref,
    dec_ref,
    bm_ref,
    cm_ref,
    wide_ref,
    x_ref,
    small_sem,
    in_sem,
    bulk_sem,
    send_sem,
    first_sem,
    part_sem,
    gated_sem,
    mixed_sem,
    square_sem,
):
    layers, groups, dp, tp, own, cols, heads, head_dim, span, features, width = dims
    me = lax.axis_index("dp")
    col = lax.axis_index("tp")
    members = dp // groups
    rows = members * own
    mine = groups - 1 - lax.rem(me, groups)
    place = me // groups

    def moved(k):
        if members & (members - 1):
            return lax.rem(place + k, members)
        return sum(
            lax.rem(place // bit + k // bit, 2) * bit
            for bit in (1 << power for power in range(members.bit_length() - 1)))

    def member(g, k):
        return moved(k) * groups + groups - 1 - g

    def slot(g, k):
        return k * groups + lax.rem(g - mine + groups, groups) - 1

    def column(k):
        return lax.rem(col + k + 1, tp)

    def columns(body):
        def at(index):
            pl.when(col + tp - index < tp)(lambda: body(col + tp - index))
            pl.when(col + index >= tp)(lambda: body(col + index - tp))

        each(tp, at, 1)

    small = [
        pltpu.make_async_copy(far, near, small_sem.at[index])
        for index, (far, near) in enumerate((
            (tokens_hbm, tokens_ref),
            (norm_hbm, norm_ref),
            (gain_hbm, gain_ref),
            (taps_hbm, taps_ref),
            (recent_hbm, recent_ref),
        ))
    ]
    heads_sem = small_sem.at[len(small)]
    per_head = [
        pltpu.make_async_copy(far, head_ref.at[index], heads_sem)
        for index, far in enumerate((bias_hbm, rate_hbm, skip_hbm))
    ]
    sources = (readout_hbm, inmap_hbm, value_hbm, gate_hbm)
    filled = step_hbm.shape[1]

    load_step = pltpu.make_async_copy(step_hbm, w_step.at[:, :filled], bulk_sem.at[0])
    load_out = pltpu.make_async_copy(project_hbm, w_out, bulk_sem.at[1])
    load_state = pltpu.make_async_copy(states_hbm, state, bulk_sem.at[2])

    def load_in(level, w):
        return pltpu.make_async_copy(
            sources[w].at[level], w_in.at[level, w], in_sem.at[w if level == 0 else level + 3])

    def await_in(level):
        pltpu.make_async_copy(w_in.at[level], w_in.at[level], in_sem.at[level + 3]).wait()

    barrier = pltpu.get_barrier_semaphore()
    each(dp, lambda k: pl.semaphore_signal(
        barrier, inc=1, device_id={"dp": lax.rem(me + k, dp)}, device_id_type=MESH), 1)
    each(tp - 1, lambda k: pl.semaphore_signal(
        barrier, inc=1, device_id={"tp": column(k)}, device_id_type=MESH))

    for copy in small[:2]:
        copy.start()
    load_step.start()
    load_in(0, 0).start()
    load_in(0, 1).start()

    def send_first(level, g, k):
        return pltpu.make_async_remote_copy(
            src_ref=first_send.at[level, g, moved(k)],
            dst_ref=first_recv.at[level, slot(g, k)],
            send_sem=send_sem.at[0],
            recv_sem=first_sem.at[level],
            device_id={"dp": member(g, k)},
            device_id_type=MESH,
        )

    def send_part(level, w, g, k):
        return pltpu.make_async_remote_copy(
            src_ref=part_send.at[level, w - 1, g, moved(k)],
            dst_ref=part_recv.at[level, w - 1, slot(g, k)],
            send_sem=send_sem.at[1],
            recv_sem=part_sem.at[level, w // GATE],
            device_id={"dp": member(g, k)},
            device_id_type=MESH,
        )

    def send_gated(level, g, k):
        return pltpu.make_async_remote_copy(
            src_ref=gated_all.at[level, mine, place],
            dst_ref=gated_all.at[level, mine, place],
            send_sem=send_sem.at[2],
            recv_sem=gated_sem.at[level, mine],
            device_id={"dp": member(g, k)},
            device_id_type=MESH,
        )

    def send_mixed(level, g, target, origin):
        return pltpu.make_async_remote_copy(
            src_ref=mixed_all.at[level, g, origin],
            dst_ref=mixed_all.at[level, g, origin],
            send_sem=send_sem.at[3],
            recv_sem=mixed_sem.at[level, g],
            device_id={"tp": target},
            device_id_type=MESH,
        )

    def send_square(level, g, target, origin):
        return pltpu.make_async_remote_copy(
            src_ref=square_all.at[level, g, origin],
            dst_ref=square_all.at[level, g, origin],
            send_sem=send_sem.at[4],
            recv_sem=square_sem.at[level, g],
            device_id={"tp": target},
            device_id_type=MESH,
        )

    def arrived(ref, sem):
        pltpu.make_async_remote_copy(
            src_ref=ref,
            dst_ref=ref,
            send_sem=send_sem.at[0],
            recv_sem=sem,
            device_id={"dp": lax.rem(me + 1, dp)},
            device_id_type=MESH,
        ).wait_recv()

    def sent(ref, index):
        pltpu.make_async_remote_copy(
            src_ref=ref,
            dst_ref=ref,
            send_sem=send_sem.at[index],
            recv_sem=first_sem.at[0],
            device_id={"dp": lax.rem(me + 1, dp)},
            device_id_type=MESH,
        ).wait_send()

    def others(which, body):
        def far(index):
            for g in which:
                body(g, members - index)

        each(members, far, 1)
        for g in which:
            if groups > 1:
                pl.when(mine != g)(functools.partial(body, g, 0))

    def every(level, w, which):
        others(which, lambda g, k: send_part(level, w, g, k).start())

    low = lax.broadcasted_iota(jnp.int32, (own, LANES), 1) < head_dim

    def twice(pair, odd):
        turned = pltpu.roll(pair, head_dim, 1)
        return jnp.where(low, turned, pair) if odd else jnp.where(low, pair, turned)

    def project_in(level, first, count):
        x = x_ref[first : first + count].reshape(count * rows, width)
        square = jnp.sum(x * x, axis=1, keepdims=True)
        gained = (x * norm_ref[level][None, :]).astype(BF16)
        lane = lax.broadcasted_iota(jnp.int32, (count * rows, LANES), 1)

        def store(w):
            part = jnp.dot(gained, w_in[level, w], preferred_element_type=F32)
            part = part.reshape(count, members, own, cols).astype(BF16)
            if w == READOUT:
                first_send[level, first : first + count, :, :, :cols] = part
            else:
                part_send[level, w - 1, first : first + count] = part

        if level == 0:
            with jax.named_scope(f"w_step_{level}"):
                load_step.wait()
        extra = lax.dot_general(
            gained, w_step[level], (((1,), (1,)), ((), ())), preferred_element_type=F32)
        extra = jnp.where(lane == LANES - 1, square, extra).reshape(count, members, own, LANES)
        high, rest = halves(extra)
        if level == 0:
            with jax.named_scope(f"w_in0_{level}"):
                load_in(level, 0).wait()
        first_send[level, first : first + count, :, :, cols : cols + LANES] = high
        first_send[level, first : first + count, :, :, cols + LANES :] = rest
        store(0)
        if level == 0 and first == 0:
            with jax.named_scope("barrier"):
                pl.semaphore_wait(barrier, dp - 1 + tp - 1)
        which = range(first, first + count)
        others(which[:1], lambda g, k: send_first(level, g, k).start())
        for w in range(1, 4):
            if level == 0:
                with jax.named_scope(f"w_in{w}_{level}"):
                    load_in(level, w).wait()
            store(w)
            with jax.named_scope(f"send{w}_{level}_{first}"):
                every(level, w, which[:1])

    def prepare():
        w_step[:, filled:] = jnp.zeros((layers, LANES - filled, width), BF16)

    def build():
        step = 256
        which = lax.broadcasted_iota(jnp.int32, (LANES, step), 0)
        entry = lax.broadcasted_iota(jnp.int32, (LANES, step), 1)
        across_lanes = lax.rem(which, head_dim) - entry // span
        which = lax.broadcasted_iota(jnp.int32, gather.shape, 1)
        entry = lax.broadcasted_iota(jnp.int32, gather.shape, 0)
        gather[...] = jnp.where(
            lax.rem(which, gather.shape[0] // span) == entry // span, 1.0, 0.0).astype(BF16)

        def fill(index, carry):
            start = pl.multiple_of(index * step, step)
            target = index * (step // span)
            spread[:, pl.ds(start, step)] = jnp.where(
                across_lanes == target, 1.0, 0.0).astype(BF16)
            return carry

        lax.fori_loop(0, head_dim * span // step, fill, 0)
        pick = lax.broadcasted_iota(jnp.int32, (LANES, cols), 0)
        slot = lax.broadcasted_iota(jnp.int32, (LANES, cols), 1)
        chosen_ref[...] = jnp.where(
            pick == col * heads + slot // head_dim, 1.0, 0.0).astype(BF16)
        pick = lax.broadcasted_iota(jnp.int32, (heads, cols), 0)
        slot = lax.broadcasted_iota(jnp.int32, (heads, cols), 1)
        wider = jnp.where(pick == slot // head_dim, 1.0, 0.0)
        for where, value in enumerate((head_ref[0], jnp.exp(head_ref[1]), head_ref[2])):
            params_ref[where] = jnp.dot(
                value, wider, preferred_element_type=F32, precision=lax.Precision.HIGHEST)

    def convolve(level):
        for j in range(3):
            conv_ref[level, j] = jnp.sum(
                recent_ref[level, :, j].astype(F32)
                * taps_ref[: taps_ref.shape[0] - 1, j, level, :].astype(F32)[None],
                axis=1,
            )

    piece = 1024
    pieces = head_dim * span // piece

    def across(ref, h):
        return jnp.concatenate([ref[h]] * (piece // LANES), axis=1)

    def mix(level):
        with jax.named_scope(f"wr_extra_{level}"):
            arrived(first_recv.at[level], first_sem.at[level])
        if level == 0:
            load_state.wait()
        both = fold(
            dp - 1,
            lambda k, sum_in: sum_in + first_recv[level, k].astype(F32),
            first_send[level, mine, place].astype(F32),
        )
        readout = both[:, :cols]
        total = both[:, cols : cols + LANES] + both[:, cols + LANES :]
        scale = lax.rsqrt(total[:, LANES - 1 :] / features + EPS)
        def total_part(w):
            return fold(
                dp - 1,
                lambda k, sum_in: sum_in + part_recv[level, w - 1, k].astype(F32),
                part_send[level, w - 1, mine, place].astype(F32),
            )

        fresh_u = {}

        def active(summed, j):
            u = (scale * summed).astype(BF16).astype(F32)
            fresh_u[j] = u
            return silu(
                conv_ref[level, j]
                + u * taps_ref[taps_ref.shape[0] - 1, j, level : level + 1, :].astype(F32))

        cm = active(readout, 2)
        for h in range(heads):
            window = slice(h // 2 * LANES, h // 2 * LANES + LANES)
            cm_ref[h] = twice(cm[:, window], h % 2)
        doubled = 2 * LANES
        chunks = head_dim * span // doubled
        read = jnp.concatenate([
            state[level, h, :, c * doubled : (c + 1) * doubled]
            * jnp.concatenate([cm_ref[h]] * 2, axis=1)
            for c in range(chunks) for h in range(heads)], axis=0).astype(BF16)
        read = jnp.dot(read, gather[...], preferred_element_type=F32)
        turn = lax.rem(
            lax.broadcasted_iota(jnp.int32, (heads * own, LANES), 1), head_dim) // (doubled // span)
        y = read[: heads * own]
        for c in range(1, chunks):
            y = jnp.where(turn == c, read[c * heads * own : (c + 1) * heads * own], y)
        chosen = chosen_ref[...]
        high, rest = halves(total * scale)
        raw = jnp.dot(high, chosen, preferred_element_type=F32) + jnp.dot(
            rest, chosen, preferred_element_type=F32)
        raw = raw + params_ref[0, level : level + 1, :]
        size = jnp.maximum(raw, 0.0) + jnp.log1p(jnp.exp(-jnp.abs(raw)))
        decay = jnp.exp(-size * params_ref[1, level : level + 1, :])

        with jax.named_scope(f"wr_part_{level}"):
            arrived(part_recv.at[level, : GATE - 1], part_sem.at[level, 0])
        bm = active(total_part(INMAP), 1)
        for h in range(heads):
            window = slice(h // 2 * LANES, h // 2 * LANES + LANES)
            dec_ref[h] = twice(decay[:, window], h % 2)
            bm_ref[h] = twice(bm[:, window], h % 2)
        xv = active(total_part(VALUE), 0)
        weighted = size * xv
        inner = []
        for h in range(heads):
            window = slice(h // 2 * LANES, h // 2 * LANES + LANES)
            one = twice(weighted[:, window], h % 2)
            high = one.astype(BF16).astype(F32)
            wide_ref[h * own : (h + 1) * own, :] = jnp.where(low, high, one - high)
            within = jnp.sum(
                jnp.where(low, bm_ref[h] * cm_ref[h], 0.0), axis=1, keepdims=True)
            inner.append(dec_ref[h] * y[h * own : (h + 1) * own] + one * within)
        y = jnp.concatenate(
            [jnp.where(low, inner[h], inner[h + 1]) for h in range(0, heads, 2)], axis=1)
        y = (y + params_ref[2, level : level + 1, :] * xv) * gain_ref[level : level + 1, :]
        with jax.named_scope(f"wr_gate_{level}"):
            arrived(part_recv.at[level, GATE - 1], part_sem.at[level, 1])
        gate = scale * total_part(GATE)
        gated_all[level, mine, place] = (y * silu(gate)).astype(BF16)
        with jax.named_scope(f"s_gated_{level}"):
            others(range(groups), lambda g, k: send_gated(level, g, k).start())
        def settle():
            with jax.named_scope(f"advance_{level}"):
                wide = wide_ref[...].astype(BF16)

                def advance(index, carry):
                    window = pl.ds(pl.multiple_of(index * piece, piece), piece)
                    grown = jnp.dot(wide, spread[:, window], preferred_element_type=F32)
                    for h in range(heads):
                        fresh_out[level, h, :, window] = (
                            across(dec_ref, h) * state[level, h, :, window]
                            + grown[h * own : (h + 1) * own] * across(bm_ref, h))
                    return carry

                lax.fori_loop(0, pieces, advance, 0)
            with jax.named_scope(f"recent_{level}"):
                for j in range(3):
                    kept = recent_ref[level, :, j].astype(F32)
                    recent_out[level, :, j] = jnp.concatenate(
                        [kept[:, 1:], fresh_u[j][:, None]], axis=1).astype(BF16)

        return settle

    cross = lax.broadcasted_iota(jnp.int32, (rows, rows), 0) == (
        lax.broadcasted_iota(jnp.int32, (rows, rows), 1))

    def project_out(level, g):
        if level == 0 and g == 0:
            load_out.wait()
        with jax.named_scope(f"wr_gated_{level}_{g}"):
            sem = gated_sem.at[level, g]
            if groups > 1:
                pl.when(mine == g)(lambda: arrived(gated_all.at[level, g, : members - 1], sem))
                pl.when(mine != g)(lambda: arrived(gated_all.at[level, g], sem))
            else:
                arrived(gated_all.at[level, g, : members - 1], sem)
        gated = gated_all[level, g].astype(F32).reshape(rows, cols)
        square = jnp.sum(gated * gated, axis=1, keepdims=True)
        square_all[level, g, col, :, :rows] = jnp.sum(
            jnp.where(cross, square, 0.0), axis=0, keepdims=True)
        mixed = jnp.dot(gated.astype(BF16), w_out[level], preferred_element_type=F32)
        mixed_all[level, g, col] = mixed.astype(BF16)
        columns(lambda target: send_square(level, g, target, col).start())
        with jax.named_scope(f"s_mixed_{level}_{g}"):
            columns(lambda target: send_mixed(level, g, target, col).start())

    def renew(level, g):
        arrived(square_all.at[level, g, : tp - 1], square_sem.at[level, g])
        square = fold(
            tp,
            lambda k, sum_in: sum_in + square_all[level, g, k, :, :rows],
            jnp.zeros((1, rows), F32),
        )
        scale = lax.rsqrt(square / (cols * tp) + EPS)
        scale = jnp.sum(jnp.where(cross, scale, 0.0), axis=1, keepdims=True)
        with jax.named_scope(f"wr_mixed_{level}_{g}"):
            arrived(mixed_all.at[level, g, : tp - 1], mixed_sem.at[level, g])
        mixed = fold(
            tp,
            lambda k, sum_in: sum_in + mixed_all[level, g, k].astype(F32),
            jnp.zeros((rows, width), F32),
        )
        fresh_x = (x_ref[g] + scale * mixed).astype(BF16)
        if level == layers - 1:
            for k in range(members):
                target = (k * groups + groups - 1 - g) * own
                tokens_out[target : target + own] = fresh_x[k * own : (k + 1) * own]
        else:
            x_ref[g] = fresh_x.astype(F32)

    prepare()
    with jax.named_scope("tokens"):
        small[0].wait()
        small[1].wait()
    load_in(0, 2).start()
    load_in(0, 3).start()
    for copy in small[2:] + per_head:
        copy.start()
    x = tokens_ref[...].astype(F32).reshape(members, groups, own, width)
    for g in range(groups):
        x_ref[g] = x[:, groups - 1 - g].reshape(rows, width)
    project_in(0, 0, groups)
    load_state.start()
    load_out.start()
    for level in range(1, layers):
        for w in range(4):
            load_in(level, w).start()
    def rest():
        if groups > 1:
            others(range(1, groups), lambda g, k: send_first(0, g, k).start())
            for w in range(1, 4):
                every(0, w, range(1, groups))

    with jax.named_scope("small_wait"):
        for copy in small[2:]:
            copy.wait()
        pltpu.make_async_copy(head_ref, head_ref, heads_sem).wait()
    with jax.named_scope("build"):
        build()
        for level in range(layers):
            convolve(level)
        rest()
    for level in range(layers):
        settle = mix(level)
        late = level < layers - 1 and groups > 1
        if not late:
            settle()
        for g in range(groups):
            project_out(level, g)
            if late and g == 0:
                settle()
        if level < layers - 1:
            await_in(level + 1)
        for g in range(groups):
            renew(level, g)
            if level < layers - 1:
                project_in(level + 1, g, 1)

    sent(first_recv, 0)
    sent(part_recv, 1)
    sent(part_recv.at[:, 0], 2)
    sent(mixed_all.at[:, :, : tp - 1], 3)
    sent(square_all.at[:, :, : tp - 1], 4)


def finish(tokens_ref, fresh_ref, recent_ref, tokens_hbm, fresh_hbm, recent_hbm, sem):
    layers, heads = fresh_ref.shape[:2]
    for level in range(layers):
        for h in range(heads):
            pltpu.make_async_copy(
                fresh_ref.at[level, h], fresh_hbm.at[level, h], sem.at[0]).start()
    small = (
        pltpu.make_async_copy(tokens_ref, tokens_hbm, sem.at[1]),
        pltpu.make_async_copy(recent_ref, recent_hbm, sem.at[2]),
    )
    for copy in small:
        copy.start()
    for copy in small:
        copy.wait()
    pltpu.make_async_copy(fresh_ref, fresh_hbm, sem.at[0]).wait()


def per_device(
    dp,
    tp,
    tokens,
    norm_gain,
    w_gate,
    w_value,
    w_inmap,
    w_readout,
    w_step,
    step_bias,
    decay_log,
    skip_gain,
    conv_taps,
    gate_gain,
    w_project,
    states,
    recent,
):
    layers, own, heads, entries = states.shape
    cols = w_gate.shape[2]
    head_dim = cols // heads
    span = entries // head_dim
    width = tokens.shape[1]
    features = width * dp
    groups = GROUPS if dp % GROUPS == 0 else 1
    dims = (layers, groups, dp, tp, own, cols, heads, head_dim, span, features, width)
    total = tokens.shape[0]
    rows = total // groups

    vmem = pl.BlockSpec(memory_space=pltpu.VMEM)
    anywhere = pl.BlockSpec(memory_space=pltpu.HBM)
    turned = recent.transpose(0, 1, 3, 2, 4)
    taps = conv_taps.transpose(1, 2, 0, 3)
    dma = pltpu.SemaphoreType.DMA
    padded = -(-rows // LANES) * LANES
    kept_bytes = 2 * tokens.size + 4 * states.size + 2 * recent.size
    results = pl.pallas_call(
        functools.partial(kernel, dims),
        out_shape=(
            pltpu.VMEM((total, width), BF16),
            pltpu.VMEM((layers, heads, own, entries), F32),
            pltpu.VMEM(turned.shape, BF16),
        ),
        in_specs=[anywhere] * 15,
        out_specs=(vmem, vmem, vmem),
        scratch_shapes=[
            pltpu.VMEM(tokens.shape, BF16),
            pltpu.VMEM(norm_gain.shape, F32),
            pltpu.VMEM((3,) + step_bias.shape, F32),
            pltpu.VMEM(gate_gain.shape, F32),
            pltpu.VMEM(taps.shape, BF16),
            pltpu.VMEM(turned.shape, BF16),
            pltpu.VMEM((layers, 4, width, cols), BF16),
            pltpu.VMEM((layers, LANES, width), BF16),
            pltpu.VMEM((layers, cols, width), BF16),
            pltpu.VMEM((layers, heads, own, entries), F32),
            pltpu.VMEM((LANES, entries), BF16),
            pltpu.VMEM((2 * LANES, LANES), BF16),
            pltpu.VMEM((layers, 3, groups, dp // groups, own, cols), BF16),
            pltpu.VMEM((layers, 3, dp - 1, own, cols), BF16),
            pltpu.VMEM((layers, groups, dp // groups, own, cols + 2 * LANES), BF16),
            pltpu.VMEM((layers, dp - 1, own, cols + 2 * LANES), BF16),
            pltpu.VMEM((layers, groups, dp // groups, own, cols), BF16),
            pltpu.VMEM((layers, groups, tp, rows, width), BF16),
            pltpu.VMEM((layers, groups, tp, 1, padded), F32),
            pltpu.VMEM((layers, 3, own, cols), F32),
            pltpu.VMEM((3, layers, cols), F32),
            pltpu.VMEM((LANES, cols), BF16),
            pltpu.VMEM((heads, own, LANES), F32),
            pltpu.VMEM((heads, own, LANES), F32),
            pltpu.VMEM((heads, own, LANES), F32),
            pltpu.VMEM((heads * own, LANES), F32),
            pltpu.VMEM((groups, rows, width), F32),
            dma((6,)),
            dma((layers + 3,)),
            dma((3,)),
            dma((5,)),
            dma((layers,)),
            dma((layers, 2)),
            dma((layers, groups)),
            dma((layers, groups)),
            dma((layers, groups)),
        ],
        compiler_params=pltpu.CompilerParams(
            collective_id=0, has_side_effects=True, vmem_limit_bytes=VMEM_BYTES - kept_bytes),
    )(
        tokens,
        norm_gain,
        step_bias,
        decay_log,
        skip_gain,
        gate_gain,
        taps,
        turned,
        w_readout,
        w_inmap,
        w_value,
        w_gate,
        w_step.transpose(0, 2, 1),
        w_project,
        states.transpose(0, 2, 1, 3),
    )
    out_tokens, fresh, kept = pl.pallas_call(
        finish,
        out_shape=(
            jax.ShapeDtypeStruct((total, width), BF16),
            jax.ShapeDtypeStruct((layers, heads, own, entries), F32),
            jax.ShapeDtypeStruct(turned.shape, BF16),
        ),
        in_specs=[vmem] * 3,
        out_specs=(anywhere,) * 3,
        scratch_shapes=[dma((3,))],
        compiler_params=pltpu.CompilerParams(vmem_limit_bytes=16 * 1024 * 1024),
    )(*results)
    next_states = fresh.transpose(0, 2, 1, 3)
    next_recent = kept.transpose(0, 1, 3, 2, 4)
    return out_tokens, next_states, next_recent


GROUPS = 2
def solution(mesh):
    in_specs = (
        P(None, "dp"),
        P(None, "dp"),
        P(None, "dp", "tp"),
        P(None, "dp", "tp"),
        P(None, "dp", "tp"),
        P(None, "dp", "tp"),
        P(None, "dp", None),
        P(None, "tp"),
        P(None, "tp"),
        P(None, "tp"),
        P(None, None, None, "tp"),
        P(None, "tp"),
        P(None, "tp", "dp"),
        P(None, "dp", "tp", None),
        P(None, "dp", None, None, "tp"),
    )
    out_specs = (P(None, "dp"), P(None, "dp", "tp", None), P(None, "dp", None, None, "tp"))
    body = functools.partial(per_device, mesh.shape["dp"], mesh.shape["tp"])
    return jax.shard_map(
        body, mesh=mesh, in_specs=in_specs, out_specs=out_specs, check_vma=False
    )
```
